128 devices in a mesh: sp: 32 (over z, y, core), tp: 4 (over x).
Axes of the slice: x: 4, y: 4, z: 4, core: 2. Of those that a mesh axis runs over, the one named last changes fastest.
Arguments:
- residual: bfloat16 [8192, 2048], P('sp'), may hold values from -6 to 6
- queries: bfloat16 [8192, 8, 2, 128], P('sp', 'tp'), may hold values from -100 to 100
- key_rows: bfloat16 [8192, 8, 2, 128], P('sp', 'tp'), may hold values from -6 to 6
- values: bfloat16 [8192, 8, 256], P('sp', 'tp'), may hold values from -6 to 6
- lambda_head: float32 [8], P('tp'), may hold values from 0.3 to 0.8
- sub_gain: float32 [256], replicated, may hold values from 0.1 to 1.9
- w_out: bfloat16 [2048, 2048], P('tp'), may hold values from -0.125 to 0.125
- norm_gain: float32 [2048], replicated, may hold values from 0.1 to 1.9
- w_gate: bfloat16 [2048, 5632], P('sp', 'tp'), may hold values from -0.125 to 0.125
- w_up: bfloat16 [2048, 5632], P('sp', 'tp'), may hold values from -0.125 to 0.125
- conv_gate: float32 [3, 5632], P(None, 'tp'), may hold values from -3 to 3
- conv_up: float32 [3, 5632], P(None, 'tp'), may hold values from -3 to 3
- w_down: bfloat16 [5632, 2048], P('tp'), may hold values from -0.078125 to 0.078125
Outputs:
- layer_out: bfloat16 [8192, 2048], P(('sp', 'tp'))
The draws below stay inside these ranges and needn't reach their ends.
All inputs are finite; a program needn't handle non-finite values.
Results may differ from the reference program's by a relative error of at most 0.017.
Values may be sent and summed in bfloat16 or wider, within the bound.
A program may use at most 192 MiB of HBM per device.

```python
import math
import jax
import jax.numpy as jnp
from jax import lax

D = 2048
HEADS = 8
DH = 128
DV = 256
FF = 5632
TOKENS = 8192


def query_key_pair(key):
    shape = (TOKENS, HEADS, 2, DH)
    keys_drawn = jnp.clip(1.3 * jax.random.normal(jax.random.fold_in(key, 12), shape, jnp.float32), -6.0, 6.0)
    queries_drawn = jnp.clip(1.3 * jax.random.normal(jax.random.fold_in(key, 11), shape, jnp.float32), -6.0, 6.0)
    return (queries_drawn, keys_drawn)


def draw_queries(key, part):
    return query_key_pair(key)[0].astype(jnp.bfloat16)


def draw_key_rows(key, part):
    return query_key_pair(key)[1].astype(jnp.bfloat16)


def block_scale(stream_key, extent, pieces, low, largest):
    def one(dim, shards_of):
        steps = jax.random.uniform(jax.random.fold_in(jax.random.fold_in(stream_key, 6), dim), (shards_of,), jnp.float32, low / len(pieces), largest / len(pieces))
        return jnp.repeat(jnp.exp(steps), extent[dim] // shards_of).reshape((-1,) + (1,) * (len(extent) - dim - 1))

    level = one(*pieces[0])
    for cut in pieces[1:]:
        level = level * one(*cut)
    return level


def normal_values(stream_key, dims, width, reach, split=(), held_as=jnp.bfloat16):
    result = width * jax.random.normal(stream_key, dims, jnp.float32)
    if split:
        result = result * block_scale(stream_key, dims, split, -0.22, 0.18)
    return jnp.clip(result, -reach, reach).astype(held_as)


def setup_inputs(seed: int = 0) -> dict:
    seeds = jax.random.split(jax.random.key(seed), 14)
    return {
        "residual": normal_values(seeds[0], (TOKENS, D), 1.0, 6.0, ((0, 32),)),
        "queries": draw_queries(jax.random.fold_in(seeds[13], 71), 0),
        "key_rows": draw_key_rows(jax.random.fold_in(seeds[13], 71), 0),
        "values": normal_values(seeds[3], (TOKENS, HEADS, DV), 1.0, 6.0, ((0, 32), (1, 4))),
        "lambda_head": jnp.clip(0.3 + 0.5 * jax.random.uniform(seeds[4], (HEADS,), jnp.float32) ** block_scale(seeds[4], (HEADS,), ((0, 4),), -0.2, 0.2), 0.3, 0.8),
        "sub_gain": jnp.clip(1.0 + 0.18 * jax.random.normal(seeds[5], (DV,), jnp.float32), 0.1, 1.9),
        "w_out": normal_values(seeds[6], (HEADS * DV, D), (HEADS * DV) ** -0.5, 0.125, ((0, 4),)),
        "norm_gain": jnp.clip(1.0 + 0.18 * jax.random.normal(seeds[7], (D,), jnp.float32), 0.1, 1.9),
        "w_gate": normal_values(seeds[8], (D, FF), D ** -0.5, 0.125, ((0, 32), (1, 4))),
        "w_up": normal_values(seeds[9], (D, FF), D ** -0.5, 0.125, ((0, 32), (1, 4))),
        "conv_gate": normal_values(seeds[10], (3, FF), 0.577, 3.0, ((1, 4),), jnp.float32),
        "conv_up": normal_values(seeds[11], (3, FF), 0.577, 3.0, ((1, 4),), jnp.float32),
        "w_down": normal_values(seeds[12], (FF, D), FF ** -0.5, 0.078125, ((0, 4),)),
    }


epsilon = 1e-06
lambda_init = 0.8 - 0.6 * math.exp(-0.3)

def causal_mix(rows_in, taps):
    padded_rows = jnp.concatenate([jnp.zeros((2, rows_in.shape[1]), jnp.float32), rows_in.astype(jnp.float32)], 0)
    return taps[0] * padded_rows[:-2] + taps[1] * padded_rows[1:-1] + taps[2] * padded_rows[2:]

def reference(residual, queries, key_rows, values, lambda_head, sub_gain, w_out, norm_gain, w_gate, w_up, conv_gate, conv_up, w_down):
    query_block = math.gcd(TOKENS, 256)
    score_scale = 1.0 / math.sqrt(DH)
    key_pos = jnp.arange(TOKENS, dtype=jnp.int32)
    keys_wide = key_rows.astype(jnp.float32)
    values_wide = values.astype(jnp.float32)

    def attend(block_start):
        query_part = lax.dynamic_slice_in_dim(queries, block_start, query_block, 0).astype(jnp.float32)
        scores = jnp.einsum('qhcd,khcd->hcqk', query_part, keys_wide) * score_scale
        query_pos = block_start + jnp.arange(query_block, dtype=jnp.int32)
        causal_mask = key_pos[None, :] <= query_pos[:, None]
        scores = jnp.where(causal_mask, scores, -1e+30)
        run_max = lax.optimization_barrier(jnp.max(scores, axis=-1, keepdims=True))
        weights = jnp.where(causal_mask, jnp.exp(scores - run_max), 0.0)
        run_sum = lax.optimization_barrier(jnp.sum(weights, axis=-1))
        rounded = lax.optimization_barrier(weights.astype(jnp.bfloat16)).astype(jnp.float32)
        summed = jnp.einsum('hcqk,khe->hcqe', rounded, values_wide)
        blended = summed / run_sum[..., None]
        return blended[:, 0] - lambda_head[:, None, None] * blended[:, 1]
    starts = (jnp.arange(TOKENS // query_block, dtype=jnp.int32) * query_block).astype(jnp.int32)
    attended = lax.map(attend, starts)
    attended = jnp.transpose(attended, (0, 2, 1, 3)).reshape(TOKENS, HEADS, DV)
    mean_square = lax.optimization_barrier(jnp.mean(attended * attended, axis=-1, keepdims=True))
    normed = attended * lax.rsqrt(mean_square + epsilon) * sub_gain * (1.0 - lambda_init)
    normed = normed.astype(jnp.bfloat16).reshape(TOKENS, HEADS * DV)
    middle = residual.astype(jnp.float32) + jnp.dot(normed, w_out, preferred_element_type=jnp.float32)
    row_square = lax.optimization_barrier(jnp.mean(middle * middle, axis=-1, keepdims=True))
    normed_rows = (middle * lax.rsqrt(row_square + epsilon) * norm_gain).astype(jnp.bfloat16)
    gate_pre = jnp.dot(normed_rows, w_gate, preferred_element_type=jnp.float32).astype(jnp.bfloat16)
    up_pre = jnp.dot(normed_rows, w_up, preferred_element_type=jnp.float32).astype(jnp.bfloat16)
    gate_mixed = causal_mix(gate_pre, conv_gate)
    up_mixed = causal_mix(up_pre, conv_up)
    hidden = (jax.nn.silu(gate_mixed) * up_mixed).astype(jnp.bfloat16)
    lowered = jnp.dot(hidden, w_down, preferred_element_type=jnp.float32)
    return (middle + lowered).astype(jnp.bfloat16)
```

```python
import functools
import math

import jax
import jax.numpy as jnp
from jax import lax
from jax.experimental import pallas as pl
from jax.experimental.pallas import tpu as pltpu
from jax.sharding import PartitionSpec as P

EPS = 1e-06
LAMBDA_INIT = 0.8 - 0.6 * math.exp(-0.3)
BF16, F32 = jnp.bfloat16, jnp.float32
MESH = pl.DeviceIdType.MESH

ORDER = (
    (0, 0),
    (1, 0), (3, 0), (0, 1), (0, 3),
    (1, 1), (1, 3), (3, 1), (3, 3),
    (2, 0), (0, 2),
    (2, 1), (2, 3), (1, 2), (3, 2),
    (2, 2),
)
STEP_OF = {d: t for t, d in enumerate(ORDER)}
FIRST = (0, 1, 3, 2)


def pick(t, values):
    return sum(jnp.where(t == i, v, 0) for i, v in enumerate(values) if v)


class Where:
    def __init__(self):
        self.sp = lax.axis_index("sp")
        self.x = lax.axis_index("tp")
        self.core = lax.rem(self.sp, 2)
        self.chip = self.sp // 2
        self.y = lax.rem(self.chip, 4)
        self.z = self.chip // 4

    def chip_behind(self, dy, dz):
        return lax.rem(self.z + 4 - dz, 4) * 4 + lax.rem(self.y + 4 - dy, 4)


class Gather:
    def __init__(self, at, buf, first, base, send, recv, dsend, drecv):
        self.at, self.buf, self.first, self.base = at, buf, first, base
        self.send, self.recv, self.dsend, self.drecv = send, recv, dsend, drecv
        self.half = buf.shape[1] // 2

    def disp(self, df, dg):
        return (df, dg) if self.first == "y" else (dg, df)

    def slot(self, df, dg):
        return self.at.chip_behind(*self.disp(df, dg)) * 2 + self.at.core

    def neighbour(self, axis, step):
        d = {1: 3, -1: 1}[step]
        return self.slot(d, 0) if axis == "f" else self.slot(0, d)

    def copy(self, ident, slot, half, to):
        ref = self.buf.at[slot]
        if half is not None:
            ref = self.buf.at[slot, pl.ds(half * self.half, self.half)]
        return pltpu.make_async_remote_copy(
            src_ref=ref, dst_ref=ref,
            send_sem=self.send.at[self.base + ident], recv_sem=self.recv.at[self.base + ident],
            device_id={"sp": to}, device_id_type=MESH,
        )

    def out(self, ident, df, dg, half, axis, step):
        self.copy(ident, self.slot(df, dg), half, self.neighbour(axis, step)).start()

    def into(self, ident, df, dg, half=None):
        self.copy(ident, self.slot(df, dg), half, self.at.sp).wait_recv()

    def across(self, df, dg):
        t = STEP_OF[self.disp(df, dg)]
        ref = self.buf.at[self.slot(df, dg)]
        self.over(t, ref).start()

    def over(self, t, ref):
        other = self.at.sp + 1 - 2 * self.at.core
        return pltpu.make_async_remote_copy(
            src_ref=ref, dst_ref=ref, send_sem=self.dsend.at[t], recv_sem=self.drecv.at[t],
            device_id={"sp": other}, device_id_type=MESH,
        )

    def from_other(self, t, chip):
        self.over(t, self.buf.at[chip * 2 + 1 - self.at.core]).wait_recv()

    def start(self):
        self.out(0, 0, 0, None, "f", 1)
        self.out(1, 0, 0, None, "f", -1)
        self.across(0, 0)
        self.out(4, 0, 0, None, "g", 1)
        self.out(5, 0, 0, None, "g", -1)

    def along_second(self, j):
        self.out(4 + 4 * j, FIRST[j], 0, None, "g", 1)
        self.out(5 + 4 * j, FIRST[j], 0, None, "g", -1)
        self.across(FIRST[j], 0)

    def got_first(self):
        self.into(0, 1, 0)
        self.out(2, 1, 0, 0, "f", 1)
        self.along_second(1)
        self.into(1, 3, 0)
        self.out(3, 3, 0, 1, "f", -1)
        self.along_second(2)

    def got_second(self, j):
        self.into(4 + 4 * j, FIRST[j], 1)
        self.out(6 + 4 * j, FIRST[j], 1, 0, "g", 1)
        self.across(FIRST[j], 1)
        self.into(5 + 4 * j, FIRST[j], 3)
        self.out(7 + 4 * j, FIRST[j], 3, 1, "g", -1)
        self.across(FIRST[j], 3)

    def got_opposite(self):
        self.into(2, 2, 0, 0)
        self.into(3, 2, 0, 1)
        self.along_second(3)

    def got_far(self, j):
        self.into(6 + 4 * j, FIRST[j], 2, 0)
        self.into(7 + 4 * j, FIRST[j], 2, 1)
        self.across(FIRST[j], 2)

    def drain(self):
        for ident in range(20):
            half = 0 if ident % 4 >= 2 else None
            self.copy(ident, self.at.sp, half, self.at.sp).wait_send()
        for t in range(16):
            self.over(t, self.buf.at[self.at.sp]).wait_send()


def kernel(
    lam, sub_gain, norm_gain, conv_g, conv_u,
    q_in, k_in, v_in, wg_in, wu_in, wo_in, wd_in, res_in,
    out,
    q, kbuf, vbuf, wg, wu, wo, wd, res,
    m_s, l_s, acc, n_loc, n_all, mid, hn, hid, head, tail, halo, part, parts,
    lsem, send, recv, dsend, drecv, xsend, xrecv, psend, precv,
):
    at = Where()
    x, sp, core = at.x, at.sp, at.core
    rows = q.shape[0]
    own = rows // 4

    loads = [
        pltpu.make_async_copy(src, dst, lsem.at[i])
        for i, (src, dst) in enumerate(
            (
                (k_in, kbuf.at[sp]), (v_in, vbuf.at[sp]), (q_in, q), (wo_in, wo.at[x]), (wg_in, wg.at[sp]),
                (wu_in, wu.at[sp]), (wd_in, wd), (res_in.at[pl.ds(x * own, own)], res),
            )
        )
    ]
    for load in loads:
        load.start()

    barrier = pltpu.get_barrier_semaphore()
    other = sp + 1 - 2 * core
    y_up, y_down = at.chip_behind(3, 0) * 2 + core, at.chip_behind(1, 0) * 2 + core
    z_up, z_down = at.chip_behind(0, 3) * 2 + core, at.chip_behind(0, 1) * 2 + core
    after, before = lax.rem(sp + 1, 32), lax.rem(sp + 31, 32)
    for to in (other, y_up, y_down, z_up, z_down, after, before):
        pl.semaphore_signal(barrier, inc=1, device_id={"sp": to}, device_id_type=MESH)
    xs = [lax.rem(x + d, 4) for d in range(4)]
    for to in xs[1:]:
        pl.semaphore_signal(barrier, inc=1, device_id={"tp": to}, device_id_type=MESH)
    pl.semaphore_wait(barrier, 10)

    keys = Gather(at, kbuf, "y", 0, send, recv, dsend.at[0], drecv.at[0])
    vals = Gather(at, vbuf, "z", 20, send, recv, dsend.at[1], drecv.at[1])
    gate = Gather(at, wg, "y", 40, send, recv, dsend.at[2], drecv.at[2])
    up = Gather(at, wu, "z", 60, send, recv, dsend.at[3], drecv.at[3])

    loads[0].wait()
    keys.start()
    loads[1].wait()
    vals.start()

    wo_half = wo.shape[1] // 2
    wo_rows = core * wo_half

    def wo_copy(ident, slot, start, size, to):
        ref = wo.at[slot, pl.ds(wo_rows + start, size)]
        return pltpu.make_async_remote_copy(
            src_ref=ref, dst_ref=ref, send_sem=xsend.at[ident], recv_sem=xrecv.at[ident],
            device_id={"tp": to}, device_id_type=MESH,
        )

    def wo_over(ident, slot, which):
        ref = wo.at[slot, pl.ds(which * wo_half, wo_half)]
        return pltpu.make_async_remote_copy(
            src_ref=ref, dst_ref=ref, send_sem=xsend.at[ident], recv_sem=xrecv.at[ident],
            device_id={"sp": other}, device_id_type=MESH,
        )

    loads[3].wait()
    wo_copy(0, x, 0, wo_half, xs[1]).start()
    wo_copy(1, x, 0, wo_half, xs[3]).start()

    def wo_middle():
        quarter = wo_half // 2
        wo_copy(0, xs[3], 0, wo_half, xs[1]).wait_recv()
        wo_copy(2, xs[3], 0, quarter, xs[1]).start()
        wo_over(4, xs[3], core).start()
        wo_copy(1, xs[1], 0, wo_half, xs[3]).wait_recv()
        wo_copy(3, xs[1], quarter, quarter, xs[3]).start()
        wo_over(5, xs[1], core).start()

    def wo_end():
        quarter = wo_half // 2
        wo_copy(2, xs[2], 0, quarter, xs[1]).wait_recv()
        wo_copy(3, xs[2], quarter, quarter, xs[3]).wait_recv()
        wo_over(6, xs[2], core).start()

    def wo_wait():
        for ident, slot in ((4, xs[3]), (5, xs[1]), (6, xs[2])):
            wo_over(ident, slot, 1 - core).wait_recv()

    loads[2].wait()

    scale = 1.0 / math.sqrt(128.0) / math.log(2.0)

    def block(chip, masked):
        for j in range(4):
            h = j // 2
            kj = kbuf[pl.ds(chip * 2, 2), :, 128 * j : 128 * j + 128].reshape(2 * rows, 128)
            vj = vbuf[pl.ds(chip * 2, 2), :, 256 * h : 256 * h + 256].reshape(2 * rows, 256)
            s = lax.dot_general(
                q[:, 128 * j : 128 * j + 128], kj, (((1,), (1,)), ((), ())), preferred_element_type=F32
            )
            s = s * scale
            if masked:
                q_pos = lax.broadcasted_iota(jnp.int32, s.shape, 0) + core * rows
                s = jnp.where(lax.broadcasted_iota(jnp.int32, s.shape, 1) <= q_pos, s, -1e30)
            top = jnp.max(s, axis=1, keepdims=True)
            if masked:
                m_new = top
            else:
                m_old = m_s[j][:, :1]
                m_new = jnp.maximum(m_old, top)
                alpha = jnp.exp2(m_old - m_new)
            p = jnp.exp2(s - m_new)
            part_sum = p[:, :128]
            for i in range(1, 2 * rows // 128):
                part_sum = part_sum + p[:, 128 * i : 128 * i + 128]
            pv = jnp.dot(p.astype(BF16), vj, preferred_element_type=F32)
            m_s[j] = jnp.broadcast_to(m_new, (rows, 128))
            if masked:
                l_s[j] = part_sum
                acc[j] = pv
            else:
                l_s[j] = l_s[j] * alpha + part_sum
                acc[j] = acc[j] * alpha + pv

    keys.from_other(0, at.chip)
    vals.from_other(0, at.chip)
    block(at.chip, True)

    def first_handler():
        keys.got_first()
        vals.got_first()
        keys.got_second(0)
        vals.got_second(0)

    def second_handler():
        keys.got_opposite()
        vals.got_opposite()
        for j in (1, 2):
            keys.got_second(j)
            vals.got_second(j)

    def third_handler():
        keys.got_far(0)
        vals.got_far(0)
        wo_middle()

    def fourth_handler():
        keys.got_second(3)
        vals.got_second(3)
        loads[4].wait()
        gate.start()
        loads[5].wait()
        up.start()
        for j in (1, 2):
            keys.got_far(j)
            vals.got_far(j)

    def fifth_handler():
        keys.got_far(3)
        vals.got_far(3)

    def step(t, carry):
        for when, handler in (
            (1, first_handler), (5, second_handler), (9, third_handler), (11, fourth_handler), (15, fifth_handler)
        ):
            pl.when(t == when)(handler)
        dy, dz = (pick(t, [d[i] for d in ORDER]) for i in (0, 1))
        chip = at.chip_behind(dy, dz)
        keys.from_other(t, chip)
        vals.from_other(t, chip)

        @pl.when(chip < at.chip)
        def _():
            block(chip, False)

        return carry

    lax.fori_loop(1, 16, step, 0)

    for h in range(2):
        mixed = []
        for c in range(2):
            j = 2 * h + c
            mixed.append(acc[j] / jnp.sum(l_s[j], axis=1, keepdims=True))
        a = mixed[0] - lam[h] * mixed[1]
        square = jnp.mean(a * a, axis=1, keepdims=True)
        n = a * lax.rsqrt(square + EPS) * sub_gain[...] * (1.0 - LAMBDA_INIT)
        n_loc[:, 256 * h : 256 * h + 256] = n.astype(BF16)

    def n_copy(d, slot, to):
        return pltpu.make_async_remote_copy(
            src_ref=n_loc.at[pl.ds(to * own, own)], dst_ref=n_all.at[slot],
            send_sem=xsend.at[6 + d], recv_sem=xrecv.at[6 + d], device_id={"tp": to}, device_id_type=MESH,
        )

    for d in range(1, 4):
        n_copy(d, x, xs[d]).start()
    n_all[pl.ds(x, 1)] = n_loc[pl.ds(pl.multiple_of(x * own, own), own), :].reshape(1, own, n_loc.shape[1])
    wo_end()
    gate.got_first()
    up.got_first()
    for d in range(1, 4):
        n_copy(d, xs[4 - d], xs[d]).wait_recv()
    wo_wait()
    loads[7].wait()

    def project(i, carry):
        cols = pl.ds(pl.multiple_of(i * 256, 256), 256)
        total = res[:, cols].astype(F32)
        for j in range(4):
            total = total + jnp.dot(n_all[j], wo[j, :, cols], preferred_element_type=F32)
        mid[:, cols] = total
        return carry

    lax.fori_loop(0, mid.shape[1] // 256, project, 0)
    middle = mid[...]
    square = jnp.mean(middle * middle, axis=1, keepdims=True)
    mine = (middle * lax.rsqrt(square + EPS) * norm_gain[...]).astype(BF16)
    hn[pl.ds(x, 1)] = mine.reshape(1, *mine.shape)

    def hn_copy(ident, slot, start, size, to):
        ref = hn.at[slot, pl.ds(start, size)]
        return pltpu.make_async_remote_copy(
            src_ref=ref, dst_ref=ref, send_sem=xsend.at[10 + ident], recv_sem=xrecv.at[10 + ident],
            device_id={"tp": to}, device_id_type=MESH,
        )

    hn_copy(0, x, 0, own, xs[1]).start()
    hn_copy(1, x, 0, own, xs[3]).start()
    gate.got_second(0)
    up.got_second(0)
    gate.got_opposite()
    up.got_opposite()
    hn_copy(0, xs[3], 0, own, xs[1]).wait_recv()
    hn_copy(2, xs[3], 0, own // 2, xs[1]).start()
    hn_copy(1, xs[1], 0, own, xs[3]).wait_recv()
    hn_copy(3, xs[1], own // 2, own // 2, xs[3]).start()
    for j in (1, 2):
        gate.got_second(j)
        up.got_second(j)
    gate.got_far(0)
    up.got_far(0)
    gate.got_second(3)
    up.got_second(3)
    hn_copy(2, xs[2], 0, own // 2, xs[1]).wait_recv()
    hn_copy(3, xs[2], own // 2, own // 2, xs[3]).wait_recv()
    for j in (1, 2, 3):
        gate.got_far(j)
        up.got_far(j)
    for t in range(16):
        chip = at.chip_behind(*ORDER[t])
        gate.from_other(t, chip)
        up.from_other(t, chip)
    loads[6].wait()

    feats = hn.shape[2]
    hidden_units = wg.shape[2]

    def mix(g, taps):
        return taps[0:1] * pltpu.roll(g, 2, 0) + taps[1:2] * pltpu.roll(g, 1, 0) + taps[2:3] * g

    def gated(gc, uc):
        return (gc * (1.0 / (1.0 + jnp.exp(-gc))) * uc).astype(BF16)

    def feed(at_col, width):
        cols = pl.ds(at_col, width)
        normed = hn[...].reshape(rows, feats)
        mixed = []
        for i, (w, taps) in enumerate(((wg, conv_g), (wu, conv_u))):
            pre = jnp.dot(normed, w[:, :, cols].reshape(feats, width), preferred_element_type=F32).astype(BF16)
            tail[i, :, cols] = pre[rows - 16 :]
            head[i, :, cols] = pre[:16]
            mixed.append(mix(pre.astype(F32), taps[:, cols]))
        hid[:, cols] = gated(*mixed)

    def feed_step(i, carry):
        feed(pl.multiple_of(i * 256, 256), 256)
        return carry

    whole = hidden_units // 256
    lax.fori_loop(0, whole, feed_step, 0)
    if hidden_units % 256:
        feed(whole * 256, hidden_units % 256)

    def halo_copy(to):
        return pltpu.make_async_remote_copy(
            src_ref=tail, dst_ref=halo, send_sem=xsend.at[14], recv_sem=xrecv.at[14],
            device_id={"sp": to}, device_id_type=MESH,
        )

    halo_copy(after).start()

    def part_copy(i, slot, to):
        cols = pl.ds(pl.multiple_of(i * 512, 512), 512)
        return pltpu.make_async_remote_copy(
            src_ref=part.at[pl.ds(to * own, own), cols], dst_ref=parts.at[slot, :, cols],
            send_sem=psend.at[to, i], recv_sem=precv.at[slot, i], device_id={"tp": to}, device_id_type=MESH,
        )

    def lower(first, last):
        def body(i, carry):
            cols = pl.ds(pl.multiple_of(i * 512, 512), 512)
            part[first * own : last * own, cols] = jnp.dot(
                hid[first * own : last * own, :], wd[:, cols], preferred_element_type=F32
            ).astype(BF16)
            for to in range(first, last):
                @pl.when(x != to)
                def _():
                    part_copy(i, x, to).start()
            return carry

        lax.fori_loop(0, part.shape[1] // 512, body, 0)

    lower(1, 4)
    halo_copy(before).wait_recv()
    mixed = []
    for i, taps in enumerate((conv_g, conv_u)):
        old = jnp.where(sp == 0, 0.0, halo[i].astype(F32))
        both = jnp.concatenate([old, head[i].astype(F32)], axis=0)
        mixed.append(mix(both, taps[...])[16:])
    hid[:16, :] = gated(*mixed)
    lower(0, 1)

    chunks = part.shape[1] // 512
    for src in range(4):
        @pl.when(x != src)
        def _():
            for i in range(chunks):
                part_copy(i, src, x).wait_recv()

        @pl.when(x == src)
        def _():
            parts[src] = part[src * own : (src + 1) * own, :]

    total = parts[0].astype(F32)
    for src in range(1, 4):
        total = total + parts[src].astype(F32)
    out[...] = (mid[...] + total).astype(BF16)

    for gather in (keys, vals, gate, up):
        gather.drain()
    quarter = wo_half // 2
    wo_copy(0, x, 0, wo_half, xs[1]).wait_send()
    wo_copy(1, x, 0, wo_half, xs[1]).wait_send()
    wo_copy(2, x, 0, quarter, xs[1]).wait_send()
    wo_copy(3, x, 0, quarter, xs[1]).wait_send()
    for ident in (4, 5, 6):
        wo_over(ident, x, core).wait_send()
    for d in range(1, 4):
        n_copy(d, x, xs[d]).wait_send()
    hn_copy(0, x, 0, own, xs[1]).wait_send()
    hn_copy(1, x, 0, own, xs[1]).wait_send()
    hn_copy(2, x, 0, own // 2, xs[1]).wait_send()
    hn_copy(3, x, 0, own // 2, xs[1]).wait_send()
    halo_copy(after).wait_send()
    for to in range(4):
        @pl.when(x != to)
        def _():
            for i in range(chunks):
                part_copy(i, x, to).wait_send()


def local(
    residual, queries, key_rows, values, lambda_head, sub_gain, w_out, norm_gain, w_gate, w_up, conv_gate, conv_up,
    w_down,
):
    rows = queries.shape[0]
    d = residual.shape[1]
    own = rows // 4
    heads_wide = queries.shape[1] * values.shape[2]
    units = w_gate.shape[1]
    maps = queries.shape[1] * 2
    places = 32
    hbm = pl.BlockSpec(memory_space=pl.ANY)
    vmem = pl.BlockSpec(memory_space=pltpu.VMEM)
    smem = pl.BlockSpec(memory_space=pltpu.SMEM)
    dma = pltpu.SemaphoreType.DMA
    call = pl.pallas_call(
        kernel,
        out_shape=jax.ShapeDtypeStruct((own, d), BF16),
        in_specs=[smem] + [vmem] * 4 + [hbm] * 8,
        out_specs=vmem,
        scratch_shapes=[
            pltpu.VMEM((rows, 512), BF16),
            pltpu.VMEM((places, rows, 512), BF16),
            pltpu.VMEM((places, rows, 512), BF16),
            pltpu.VMEM((places, w_gate.shape[0], units), BF16),
            pltpu.VMEM((places, w_gate.shape[0], units), BF16),
            pltpu.VMEM((4, *w_out.shape), BF16),
            pltpu.VMEM(w_down.shape, BF16),
            pltpu.VMEM((own, d), BF16),
            pltpu.VMEM((maps, rows, 128), F32),
            pltpu.VMEM((maps, rows, 128), F32),
            pltpu.VMEM((maps, rows, values.shape[2]), F32),
            pltpu.VMEM((rows, heads_wide), BF16),
            pltpu.VMEM((4, own, heads_wide), BF16),
            pltpu.VMEM((own, d), F32),
            pltpu.VMEM((4, own, d), BF16),
            pltpu.VMEM((rows, units), BF16),
            pltpu.VMEM((2, 16, units), BF16),
            pltpu.VMEM((2, 16, units), BF16),
            pltpu.VMEM((2, 16, units), BF16),
            pltpu.VMEM((rows, d), BF16),
            pltpu.VMEM((4, own, d), BF16),
            dma((8,)), dma((80,)), dma((80,)), dma((4, 16)), dma((4, 16)), dma((16,)), dma((16,)),
            dma((4, d // 512)), dma((4, d // 512)),
        ],
        compiler_params=pltpu.CompilerParams(
            collective_id=0, has_side_effects=True, vmem_limit_bytes=67043328
        ),
    )
    return call(
        lambda_head, sub_gain[None], norm_gain[None], conv_gate, conv_up,
        queries.reshape(rows, 512), key_rows.reshape(rows, 512), values.reshape(rows, 512),
        w_gate, w_up, w_out, w_down, residual,
    )


def solution(mesh):
    placed = (
        P("sp", None),
        P("sp", "tp", None, None),
        P("sp", "tp", None, None),
        P("sp", "tp", None),
        P("tp"),
        P(),
        P("tp", None),
        P(),
        P("sp", "tp"),
        P("sp", "tp"),
        P(None, "tp"),
        P(None, "tp"),
        P("tp", None),
    )
    return jax.shard_map(
        local, mesh=mesh, in_specs=placed, out_specs=P(("sp", "tp"), None), check_vma=False
    )
```

```python
import functools
import math

import jax
import jax.numpy as jnp
from jax import lax
from jax.experimental import pallas as pl
from jax.experimental.pallas import tpu as pltpu
from jax.sharding import PartitionSpec as P

EPS = 1e-06
LAMBDA_INIT = 0.8 - 0.6 * math.exp(-0.3)
BF16, F32 = jnp.bfloat16, jnp.float32
MESH = pl.DeviceIdType.MESH

ORDER = (
    (0, 0),
    (1, 0), (3, 0), (0, 1), (0, 3),
    (1, 1), (1, 3), (3, 1), (3, 3),
    (2, 0), (0, 2),
    (2, 1), (2, 3), (1, 2), (3, 2),
    (2, 2),
)
STEP_OF = {d: t for t, d in enumerate(ORDER)}
FIRST = (0, 1, 3, 2)
HALF_ORDER = ((0, 0), (1, 0), (3, 0), (0, 1), (2, 0), (1, 1), (3, 1), (2, 1))
HALF_STEP_OF = {d: t for t, d in enumerate(HALF_ORDER)}


def pick(t, values):
    return sum(jnp.where(t == i, v, 0) for i, v in enumerate(values) if v)


def remote(src, dst, send, recv, **to):
    return pltpu.make_async_remote_copy(
        src_ref=src, dst_ref=dst, send_sem=send, recv_sem=recv, device_id=to, device_id_type=MESH
    )


class Where:
    def __init__(self):
        self.sp = lax.axis_index("sp")
        self.x = lax.axis_index("tp")
        self.core = lax.rem(self.sp, 2)
        self.other = self.sp + 1 - 2 * self.core
        self.chip = self.sp // 2
        self.y = lax.rem(self.chip, 4)
        self.z = self.chip // 4
        self.zl = lax.rem(self.z, 2)
        self.late = self.z // 2

    def chip_behind(self, dy, dz):
        return lax.rem(self.z + 4 - dz, 4) * 4 + lax.rem(self.y + 4 - dy, 4)

    def step(self, axis, forward):
        d = 3 if forward else 1
        return (self.chip_behind(d, 0) if axis == "y" else self.chip_behind(0, d)) * 2 + self.core

    def pair(self):
        return ((self.z + 1 - 2 * self.zl) * 4 + self.y) * 2 + self.core

    def opposite(self):
        return ((3 - self.z) * 4 + self.y) * 2 + self.core

    def half_chip(self, dy, zo):
        zl = self.zl + zo - 2 * zo * self.zl
        return zl * 4 + lax.rem(self.y + 4 - dy, 4)


class Gather:
    def __init__(self, at, buf, first, send, recv, drecv):
        self.at, self.buf, self.send, self.recv, self.drecv = at, buf, send, recv, drecv
        self.axes = {"f": first, "g": "z" if first == "y" else "y"}
        self.half = buf.shape[1] // 2

    def slot(self, df, dg):
        dy, dz = (df, dg) if self.axes["f"] == "y" else (dg, df)
        return self.at.chip_behind(dy, dz) * 2 + self.at.core

    def copy(self, ident, slot, half, to):
        ref = self.buf.at[slot]
        if half is not None:
            ref = self.buf.at[slot, pl.ds(half * self.half, self.half)]
        return remote(ref, ref, self.send, self.recv.at[ident], sp=to)

    def out(self, ident, df, dg, half, axis, forward):
        self.copy(ident, self.slot(df, dg), half, self.at.step(self.axes[axis], forward)).start()

    def into(self, ident, df, dg):
        self.copy(ident, self.slot(df, dg), None, self.at.other).wait_recv()

    def across(self, df, dg):
        ref = self.buf.at[self.slot(df, dg)]
        remote(ref, ref, self.send, self.drecv, sp=self.at.other).start()

    def start_along(self, axis, forward):
        self.out((0 if axis == "f" else 3) + (not forward), 0, 0, None, axis, forward)

    def along_second(self, j):
        self.second_step(j, True)
        self.second_step(j, False)
        self.across(FIRST[j], 0)

    def second_step(self, j, forward):
        self.out((3 if forward else 4) + 3 * j, FIRST[j], 0, None, "g", forward)

    def got_first(self):
        self.into(0, 1, 0)
        self.into(1, 3, 0)

    def first_step(self, forward):
        if forward:
            self.out(2, 1, 0, 0, "f", True)
        else:
            self.out(2, 3, 0, 1, "f", False)

    def got_second(self, j):
        self.into(3 + 3 * j, FIRST[j], 1)
        self.out(5 + 3 * j, FIRST[j], 1, 0, "g", True)
        self.into(4 + 3 * j, FIRST[j], 3)
        self.out(5 + 3 * j, FIRST[j], 3, 1, "g", False)
        self.across(FIRST[j], 1)
        self.across(FIRST[j], 3)

    def got_opposite(self):
        self.into(2, 2, 0)
        self.along_second(3)

    def got_far(self, j):
        self.into(5 + 3 * j, FIRST[j], 2)
        self.across(FIRST[j], 2)

    def from_other(self):
        ref = self.buf.at[pl.ds(0, 16)]
        remote(ref, ref, self.send, self.drecv, sp=self.at.other).wait_recv()

    def drain(self):
        ref = self.buf.at[pl.ds(0, 31)]
        remote(ref, ref, self.send, self.drecv, sp=self.at.other).wait_send()


class HalfGather:
    def __init__(self, at, buf, send, recv, drecv):
        self.at, self.buf, self.send, self.recv, self.drecv = at, buf, send, recv, drecv
        self.half = buf.shape[1] // 2

    def slot(self, dy, zo):
        return self.at.half_chip(dy, zo) * 2 + self.at.core

    def copy(self, ident, dy, zo, half, to):
        ref = self.buf.at[self.slot(dy, zo)]
        if half is not None:
            ref = self.buf.at[self.slot(dy, zo), pl.ds(half * self.half, self.half)]
        return remote(ref, ref, self.send, self.recv.at[ident], sp=to)

    def out(self, ident, dy, zo, half, to):
        self.copy(ident, dy, zo, half, to).start()

    def into(self, ident, dy, zo):
        self.copy(ident, dy, zo, None, self.at.other).wait_recv()

    def over(self, t, slot):
        ref = self.buf.at[slot]
        return remote(ref, ref, self.send, self.drecv.at[t], sp=self.at.other)

    def across(self, dy, zo):
        self.over(HALF_STEP_OF[dy, zo], self.slot(dy, zo)).start()

    def from_other(self, t, chip):
        self.over(t, chip * 2 + 1 - self.at.core).wait_recv()

    def ring_start(self, ident, zo):
        self.out(ident, 0, zo, None, self.at.step("y", True))
        self.out(ident + 1, 0, zo, None, self.at.step("y", False))

    def ring_middle(self, ident, zo, after=lambda dy: None):
        self.into(ident, 1, zo)
        self.out(ident + 2, 1, zo, 0, self.at.step("y", True))
        after(1)
        self.across(1, zo)
        self.into(ident + 1, 3, zo)
        self.out(ident + 2, 3, zo, 1, self.at.step("y", False))
        after(3)
        self.across(3, zo)

    def ring_end(self, ident, zo, after=lambda dy: None):
        self.into(ident + 2, 2, zo)
        after(2)
        self.across(2, zo)

    def drain(self):
        ref = self.buf.at[pl.ds(0, 15)]
        remote(ref, ref, self.send, self.recv.at[0], sp=self.at.other).wait_send()


def kernel(
    lam, sub_gain, norm_gain, conv_g, conv_u,
    q_in, k_in, v_in, wg_in, wu_in, wo_in, wd_in, res_in,
    out,
    q_raw, k_raw, v_raw, q, kbuf, vbuf, wg, wu, wo, wd, res,
    m_s, l_s, acc, a_far, stat, stat_far, n_loc, n_all, mid, hn, hid, part, relay, parts,
    lsem, send, krecv, kdrecv, wrecv, drecv, orecv, xrecv, precv,
):
    at = Where()
    x, sp, core, other = at.x, at.sp, at.core, at.other
    rows = q.shape[1]
    own = rows // 4
    late = at.late == 1
    early = at.late == 0
    mine = at.half_chip(0, 0)

    loads = [
        pltpu.make_async_copy(src, dst, lsem.at[i])
        for i, (src, dst) in enumerate(
            (
                (k_in, k_raw), (v_in, v_raw), (q_in, q_raw), (wo_in, wo.at[x]),
                (wg_in, wg.at[sp]), (wu_in, wu.at[sp]), (wd_in, wd), (res_in.at[pl.ds(x * own, own)], res),
            )
        )
    ]
    for load in loads:
        load.start()

    barrier = pltpu.get_barrier_semaphore()
    after, before = lax.rem(sp + 1, 32), lax.rem(sp + 31, 32)
    for to in (
        other, at.step("y", True), at.step("y", False), at.step("z", True), at.step("z", False), after, before
    ):
        pl.semaphore_signal(barrier, inc=1, device_id={"sp": to}, device_id_type=MESH)
    xs = [lax.rem(x + d, 4) for d in range(4)]
    for to in xs[1:]:
        pl.semaphore_signal(barrier, inc=1, device_id={"tp": to}, device_id_type=MESH)
    for load, raw, laid in (
        (loads[0], k_raw, kbuf.at[mine * 2 + core]), (loads[1], v_raw, vbuf.at[mine * 2 + core]), (loads[2], q_raw, q.at[0])
    ):
        load.wait()
        laid[...] = raw[...].reshape(laid.shape)
    with jax.named_scope("barrier"):
        pl.semaphore_wait(barrier, 10)

    keys = HalfGather(at, kbuf, send.at[0], krecv.at[0], kdrecv.at[0])
    vals = HalfGather(at, vbuf, send.at[1], krecv.at[1], kdrecv.at[1])
    gate = Gather(at, wg, "y", send.at[2], wrecv.at[0], drecv.at[0])
    up = Gather(at, wu, "z", send.at[3], wrecv.at[1], drecv.at[1])

    def key_on(dy):
        keys.out(3 + FIRST.index(dy), dy, 0, None, at.pair())

    def q_copy():
        return remote(q.at[0], q.at[1], send.at[9], orecv.at[0], sp=at.opposite())

    keys.ring_start(0, 0)
    vals.out(0, 0, 0, None, at.pair())
    key_on(0)
    vals.ring_start(1, 0)
    keys.across(0, 0)
    vals.across(0, 0)

    @pl.when(late)
    def _():
        q_copy().start()

    def weights_along_z(forward):
        gate.start_along("g", forward)
        up.start_along("f", forward)

    loads[4].wait()
    loads[5].wait()
    for forward in (True, False):
        pl.when(at.zl == int(forward))(functools.partial(weights_along_z, forward))

    def weights_start():
        for forward in (True, False):
            gate.start_along("f", forward)
            up.start_along("g", forward)
            pl.when(at.zl == int(not forward))(functools.partial(weights_along_z, forward))
        gate.across(0, 0)
        up.across(0, 0)

    wo_half = wo.shape[1] // 2
    wo_quarter = wo_half // 2

    def wo_copy(ident, slot, start, size, to):
        ref = wo.at[slot, pl.ds(core * wo_half + start, size)]
        return remote(ref, ref, send.at[4], xrecv.at[ident], tp=to)

    def wo_over(slot):
        ref = wo.at[slot, pl.ds(core * wo_half, wo_half)]
        return remote(ref, ref, send.at[4], xrecv.at[3], sp=other)

    loads[3].wait()
    wo_copy(0, x, 0, wo_half, xs[1]).start()
    wo_copy(1, x, 0, wo_half, xs[3]).start()

    def wo_middle():
        wo_copy(0, xs[3], 0, wo_half, xs[1]).wait_recv()
        wo_copy(2, xs[3], 0, wo_quarter, xs[1]).start()
        wo_over(xs[3]).start()
        wo_copy(1, xs[1], 0, wo_half, xs[3]).wait_recv()
        wo_copy(2, xs[1], wo_quarter, wo_quarter, xs[3]).start()
        wo_over(xs[1]).start()

    def wo_end():
        wo_copy(2, xs[2], 0, wo_half, xs[1]).wait_recv()
        wo_over(xs[2]).start()

    def wo_wait():
        ref = wo.at[pl.ds(0, 3), pl.ds(0, wo_half)]
        remote(ref, ref, send.at[4], xrecv.at[3], sp=other).wait_recv()

    scale = 1.0 / math.sqrt(128.0) / math.log(2.0)

    def block(who, chip, masked):
        for j in range(4):
            h = j // 2
            kj = kbuf[pl.ds(chip * 2, 2), :, 128 * j : 128 * j + 128].reshape(2 * rows, 128)
            vj = vbuf[pl.ds(chip * 2, 2), :, 256 * h : 256 * h + 256].reshape(2 * rows, 256)
            s = lax.dot_general(
                q[who, :, 128 * j : 128 * j + 128], kj, (((1,), (1,)), ((), ())), preferred_element_type=F32
            )
            s = s * scale
            if masked:
                q_pos = lax.broadcasted_iota(jnp.int32, s.shape, 0) + core * rows
                s = jnp.where(lax.broadcasted_iota(jnp.int32, s.shape, 1) <= q_pos, s, -1e30)
            top = jnp.max(s, axis=1, keepdims=True)
            if masked:
                m_new = top
            else:
                m_old = m_s[4 * who + j][:, :1]
                m_new = jnp.maximum(m_old, top)
                alpha = jnp.exp2(m_old - m_new)
            p = jnp.exp2(s - m_new)
            part_sum = p[:, :128]
            for i in range(1, 2 * rows // 128):
                part_sum = part_sum + p[:, 128 * i : 128 * i + 128]
            pv = jnp.dot(p.astype(BF16), vj, preferred_element_type=F32)
            m_s[4 * who + j] = jnp.broadcast_to(m_new, (rows, 128))
            if masked:
                l_s[4 * who + j] = part_sum
                acc[4 * who + j] = pv
            else:
                l_s[4 * who + j] = l_s[4 * who + j] * alpha + part_sum
                acc[4 * who + j] = acc[4 * who + j] * alpha + pv

    @pl.when(early)
    def _():
        m_s[4:] = jnp.full((4, rows, 128), -1e30, F32)
        l_s[4:] = jnp.zeros((4, rows, 128), F32)
        acc[4:] = jnp.zeros((4, *acc.shape[1:]), F32)

    with jax.named_scope("own_wait"):
        keys.from_other(0, mine)
        vals.from_other(0, mine)
    with jax.named_scope("own_block"):
        block(0, mine, True)

    def handler_0():
        keys.ring_middle(0, 0, key_on)
        vals.into(0, 0, 1)
        vals.ring_start(4, 1)
        vals.across(0, 1)
        vals.ring_middle(1, 0)
        keys.into(3, 0, 1)
        keys.across(0, 1)

        @pl.when(early)
        def _():
            q_copy().wait_recv()

    def handler_2():
        keys.ring_end(0, 0, key_on)

    def handler_4():
        vals.ring_middle(4, 1)
        weights_start()
        vals.ring_end(1, 0)

    def handler_5():
        keys.into(4, 1, 1)
        keys.across(1, 1)
        keys.into(5, 3, 1)
        keys.across(3, 1)

    def handler_7():
        vals.ring_end(4, 1)
        keys.into(6, 2, 1)
        keys.across(2, 1)
        wo_middle()

    def step(t, carry):
        for when, handler in (
            (0, handler_0), (2, handler_2), (4, handler_4), (5, handler_5), (7, handler_7)
        ):

            @pl.when(t == when)
            def _():
                with jax.named_scope(handler.__name__):
                    handler()

        dy, zo = (pick(t, [d[i] for d in HALF_ORDER]) for i in (0, 1))
        chip = at.half_chip(dy, zo)

        @pl.when(t > 0)
        def _():
            with jax.named_scope("d2d_wait"):
                keys.from_other(t, chip)
                vals.from_other(t, chip)

        @pl.when(early)
        def _():
            with jax.named_scope("far_block"):
                block(1, chip, False)

        @pl.when(chip < mine)
        def _():
            with jax.named_scope("block"):
                block(0, chip, False)

        return carry

    lax.fori_loop(0, 8, step, 0)

    def stat_copy():
        return remote(stat, stat_far, send.at[10], orecv.at[1], sp=at.opposite())

    def a_copy(h):
        return remote(a_far.at[h], a_far.at[h], send.at[11], orecv.at[2 + h], sp=at.opposite())

    lanes = lax.broadcasted_iota(jnp.int32, (rows, 128), 1)
    base = 4 - 4 * at.late
    stats = jnp.zeros((rows, 128), F32)
    for j in range(4):
        total = jnp.sum(l_s[base + j], axis=1, keepdims=True)
        stats = jnp.where(lanes == j, m_s[base + j], jnp.where(lanes == 4 + j, total, stats))
    stat[...] = stats.T[:8]
    stat_copy().start()

    def weights_on_along_z(forward):
        up.first_step(forward)
        gate.second_step(1, forward)
        gate.second_step(2, forward)

    with jax.named_scope("w_first"):
        gate.got_first()
        for forward in (True, False):
            gate.first_step(forward)
        up.got_first()
        for forward in (True, False):
            pl.when(at.zl == int(not forward))(functools.partial(weights_on_along_z, forward))
        for j in (1, 2):
            up.along_second(j)
            gate.across(FIRST[j], 0)

    with jax.named_scope("stat_wait"):
        stat_copy().wait_recv()

    with jax.named_scope("blend"):
        here = jnp.concatenate([stat[...], jnp.zeros((120, rows), F32)], axis=0).T
        there = jnp.concatenate([stat_far[...], jnp.zeros((120, rows), F32)], axis=0).T
        for h in range(2):
            shares = []
            for j in (2 * h, 2 * h + 1):
                m_here, m_there = here[:, j : j + 1], there[:, j : j + 1]
                top = jnp.maximum(m_here, m_there)
                e_here, e_there = jnp.exp2(m_here - top), jnp.exp2(m_there - top)
                total = here[:, 4 + j : 5 + j] * e_here + there[:, 4 + j : 5 + j] * e_there
                shares.append(acc[base + j] * (e_here / total))
            a = shares[0] - lam[h] * shares[1]

            @pl.when(early)
            def _():
                a_far[h] = a.astype(BF16)
                a_copy(h).start()

            @pl.when(late)
            def _():
                acc[2 * h] = a

    for forward in (True, False):
        pl.when(at.zl == int(forward))(functools.partial(weights_on_along_z, forward))

    with jax.named_scope("w_second"):
        gate.got_second(0)
        up.got_second(0)
        gate.got_opposite()
        up.got_opposite()

    for h in range(2):

        @pl.when(late)
        def _():
            with jax.named_scope("a_wait"):
                a_copy(h).wait_recv()
            acc[2 * h] = acc[2 * h] + a_far[h].astype(F32)

        @pl.when(early)
        def _():
            mixed = []
            for j in (2 * h, 2 * h + 1):
                mixed.append(acc[j] / jnp.sum(l_s[j], axis=1, keepdims=True))
            acc[2 * h] = mixed[0] - lam[h] * mixed[1]

        a = acc[2 * h]
        square = jnp.mean(a * a, axis=1, keepdims=True)
        n = a * lax.rsqrt(square + EPS) * sub_gain[...] * (1.0 - LAMBDA_INIT)
        n_loc[:, 256 * h : 256 * h + 256] = n.astype(BF16)

    def n_copy(d, slot, to):
        return remote(n_loc.at[pl.ds(to * own, own)], n_all.at[slot], send.at[5], xrecv.at[4 + d], tp=to)

    for d in range(1, 4):
        n_copy(d, x, xs[d]).start()
    n_all[pl.ds(x, 1)] = n_loc[pl.ds(pl.multiple_of(x * own, own), own), :].reshape(1, own, n_loc.shape[1])
    with jax.named_scope("wo_end"):
        wo_end()
    with jax.named_scope("w_third"):
        for j in (1, 2):
            gate.got_second(j)
            up.got_second(j)
    with jax.named_scope("n_wait"):
        for d in range(1, 4):
            n_copy(d, xs[4 - d], xs[d]).wait_recv()
    with jax.named_scope("wo_wait"):
        wo_wait()
        loads[7].wait()

    def project(i, carry):
        cols = pl.ds(pl.multiple_of(i * 256, 256), 256)
        total = res[:, cols].astype(F32)
        for j in range(4):
            total = total + jnp.dot(n_all[j], wo[j, :, cols], preferred_element_type=F32)
        mid[:, cols] = total
        return carry

    with jax.named_scope("project"):
        lax.fori_loop(0, mid.shape[1] // 256, project, 0, unroll=True)
    middle = mid[...]
    square = jnp.mean(middle * middle, axis=1, keepdims=True)

    def hn_at(slot, start, size):
        return pl.ds(pl.multiple_of(16 + slot * own + start, 16), size)

    hn[hn_at(x, 0, own), :] = (middle * lax.rsqrt(square + EPS) * norm_gain[...]).astype(BF16)

    def hn_copy(ident, slot, start, size, to):
        ref = hn.at[hn_at(slot, start, size)]
        return remote(ref, ref, send.at[6], xrecv.at[8 + ident], tp=to)

    def halo_copy(to):
        return remote(hn.at[pl.ds(rows, 16)], hn.at[pl.ds(0, 16)], send.at[7], xrecv.at[11], sp=to)

    hn_copy(0, x, 0, own, xs[1]).start()
    hn_copy(1, x, 0, own, xs[3]).start()
    with jax.named_scope("w_fourth"):
        gate.got_second(3)
        up.got_second(3)
    with jax.named_scope("hn_middle"):
        hn_copy(0, xs[3], 0, own, xs[1]).wait_recv()
        hn_copy(2, xs[3], 0, own // 2, xs[1]).start()
        hn_copy(1, xs[1], 0, own, xs[3]).wait_recv()
        hn_copy(2, xs[1], own // 2, own // 2, xs[3]).start()
    with jax.named_scope("w_fifth"):
        for j in range(4):
            gate.got_far(j)
            up.got_far(j)
    with jax.named_scope("hn_wait"):
        hn_copy(2, xs[2], 0, own, xs[1]).wait_recv()
    pl.when(sp < 31)(lambda: halo_copy(after).start())
    with jax.named_scope("w_over"):
        gate.from_other()
        up.from_other()
        loads[6].wait()

    @pl.when(sp > 0)
    def _():
        with jax.named_scope("halo_wait"):
            halo_copy(before).wait_recv()

    @pl.when(sp == 0)
    def _():
        hn[:16, :] = jnp.zeros((16, hn.shape[1]), BF16)


    feats = hn.shape[1]
    units = wg.shape[2]

    def mix(g, taps):
        return taps[0:1] * pltpu.roll(g, 2, 0) + taps[1:2] * pltpu.roll(g, 1, 0) + taps[2:3] * g

    def feed(at_col, width):
        cols = pl.ds(at_col, width)
        mixed = []
        for w, taps in ((wg, conv_g), (wu, conv_u)):
            pre = jnp.dot(hn[...], w[:, :, cols].reshape(feats, width), preferred_element_type=F32)
            mixed.append(mix(pre.astype(BF16).astype(F32), taps[:, cols])[16:])
        gc, uc = mixed
        hid[:, cols] = (gc * (1.0 / (1.0 + jnp.exp(-gc))) * uc).astype(BF16)

    def feed_step(i, carry):
        feed(pl.multiple_of(i * 256, 256), 256)
        return carry

    whole = units // 256
    with jax.named_scope("feed"):
        lax.fori_loop(0, whole, feed_step, 0, unroll=True)
        if units % 256:
            feed(whole * 256, units % 256)

    chunks = part.shape[2] // 512
    side = own // 2

    def cols_of(i):
        return pl.ds(pl.multiple_of(i * 512, 512), 512)

    def relay_copy(s, i, to):
        return remote(
            part.at[xs[2], pl.ds(s * side, side), cols_of(i)], relay.at[s, :, cols_of(i)],
            send.at[8], precv.at[0, s, i], tp=to,
        )

    def part_copy(s, i, to):
        return remote(
            part.at[to, :, cols_of(i)], parts.at[s, :, cols_of(i)], send.at[8], precv.at[1, s, i], tp=to
        )

    def lower(i, carry):
        cols = cols_of(i)
        full = jnp.dot(hid[...], wd[:, cols], preferred_element_type=F32).astype(BF16)
        part[:, :, cols] = full.reshape(4, own, 512)
        relay_copy(0, i, xs[1]).start()
        relay_copy(1, i, xs[3]).start()
        return carry

    with jax.named_scope("lower"):
        lax.fori_loop(0, chunks, lower, 0, unroll=True)

    def pass_on(i, carry):
        cols = cols_of(i)
        for s, to in ((0, xs[1]), (1, xs[3])):
            relay_copy(s, i, to).wait_recv()
            half = pl.ds(s * side, side)
            total = part[to, half, cols].astype(F32) + relay[s, :, cols].astype(F32)
            part[to, half, cols] = total.astype(BF16)
            part_copy(s, i, to).start()
        return carry

    with jax.named_scope("pass_on"):
        lax.fori_loop(0, chunks, pass_on, 0)

    def finish(i, carry):
        cols = cols_of(i)
        for s, to in ((0, xs[1]), (1, xs[3])):
            part_copy(s, i, to).wait_recv()
        total = parts[0, :, cols].astype(F32) + parts[1, :, cols].astype(F32) + part[x, :, cols].astype(F32)
        out[:, cols] = (mid[:, cols] + total).astype(BF16)
        return carry

    with jax.named_scope("finish"):
        lax.fori_loop(0, chunks, finish, 0)

    def sent(ref, which):
        remote(ref, ref, send.at[which], xrecv.at[0], sp=other).wait_send()

    with jax.named_scope("drain"):
        for gather in (keys, vals, gate, up):
            gather.drain()
        sent(wo.at[pl.ds(0, 3)], 4)
        sent(n_all.at[pl.ds(0, 3)], 5)
        sent(hn.at[pl.ds(0, 3 * own)], 6)
        pl.when(sp < 31)(lambda: halo_copy(after).wait_send())
        sent(hn.at[pl.ds(0, 3 * own)], 8)
        stat_copy().wait_send()

        @pl.when(late)
        def _():
            q_copy().wait_send()

        @pl.when(early)
        def _():
            sent(a_far, 11)


def local(
    residual, queries, key_rows, values, lambda_head, sub_gain, w_out, norm_gain, w_gate, w_up, conv_gate, conv_up,
    w_down,
):
    rows = queries.shape[0]
    d = residual.shape[1]
    own = rows // 4
    heads_wide = queries.shape[1] * values.shape[2]
    units = w_gate.shape[1]
    maps = queries.shape[1] * 2
    places = 32
    hbm = pl.BlockSpec(memory_space=pl.ANY)
    vmem = pl.BlockSpec(memory_space=pltpu.VMEM)
    smem = pl.BlockSpec(memory_space=pltpu.SMEM)
    dma = pltpu.SemaphoreType.DMA
    call = pl.pallas_call(
        kernel,
        out_shape=jax.ShapeDtypeStruct((own, d), BF16),
        in_specs=[smem] + [vmem] * 4 + [hbm] * 8,
        out_specs=vmem,
        scratch_shapes=[
            pltpu.VMEM(queries.shape, BF16),
            pltpu.VMEM(key_rows.shape, BF16),
            pltpu.VMEM(values.shape, BF16),
            pltpu.VMEM((2, rows, 512), BF16),
            pltpu.VMEM((places // 2, rows, 512), BF16),
            pltpu.VMEM((places // 2, rows, 512), BF16),
            pltpu.VMEM((places, w_gate.shape[0], units), BF16),
            pltpu.VMEM((places, w_gate.shape[0], units), BF16),
            pltpu.VMEM((4, *w_out.shape), BF16),
            pltpu.VMEM(w_down.shape, BF16),
            pltpu.VMEM((own, d), BF16),
            pltpu.VMEM((2 * maps, rows, 128), F32),
            pltpu.VMEM((2 * maps, rows, 128), F32),
            pltpu.VMEM((2 * maps, rows, values.shape[2]), F32),
            pltpu.VMEM((2, rows, values.shape[2]), BF16),
            pltpu.VMEM((8, rows), F32),
            pltpu.VMEM((8, rows), F32),
            pltpu.VMEM((rows, heads_wide), BF16),
            pltpu.VMEM((4, own, heads_wide), BF16),
            pltpu.VMEM((own, d), F32),
            pltpu.VMEM((rows + 16, d), BF16),
            pltpu.VMEM((rows, units), BF16),
            pltpu.VMEM((4, own, d), BF16),
            pltpu.VMEM((2, own // 2, d), BF16),
            pltpu.VMEM((2, own, d), BF16),
            dma((8,)), dma((12,)), dma((2, 7)), dma((2, 8)), dma((2, 15)), dma((2,)), dma((4,)), dma((12,)),
            dma((2, 2, d // 512)),
        ],
        compiler_params=pltpu.CompilerParams(
            collective_id=0, has_side_effects=True, vmem_limit_bytes=67043328
        ),
    )
    return call(
        lambda_head, sub_gain[None], norm_gain[None], conv_gate, conv_up,
        queries, key_rows, values,
        w_gate, w_up, w_out, w_down, residual,
    )


def solution(mesh):
    placed = (
        P("sp", None),
        P("sp", "tp", None, None),
        P("sp", "tp", None, None),
        P("sp", "tp", None),
        P("tp"),
        P(),
        P("tp", None),
        P(),
        P("sp", "tp"),
        P("sp", "tp"),
        P(None, "tp"),
        P(None, "tp"),
        P("tp", None),
    )
    return jax.shard_map(
        local, mesh=mesh, in_specs=placed, out_specs=P(("sp", "tp"), None), check_vma=False
    )
```

```python
import functools
import math

import jax
import jax.numpy as jnp
from jax import lax
from jax.experimental import pallas as pl
from jax.experimental.pallas import tpu as pltpu
from jax.sharding import PartitionSpec as P

EPS = 1e-06
LAMBDA_INIT = 0.8 - 0.6 * math.exp(-0.3)
BF16, F32 = jnp.bfloat16, jnp.float32
MESH = pl.DeviceIdType.MESH

ORDER = (
    (0, 0),
    (1, 0), (3, 0), (0, 1), (0, 3),
    (1, 1), (1, 3), (3, 1), (3, 3),
    (2, 0), (0, 2),
    (2, 1), (2, 3), (1, 2), (3, 2),
    (2, 2),
)
STEP_OF = {d: t for t, d in enumerate(ORDER)}
FIRST = (0, 1, 3, 2)
HALF_ORDER = ((0, 0), (1, 0), (3, 0), (0, 1), (1, 1), (3, 1), (2, 0), (2, 1))
HALF_STEP_OF = {d: t for t, d in enumerate(HALF_ORDER)}


def pick(t, values):
    return sum(jnp.where(t == i, v, 0) for i, v in enumerate(values) if v)


def remote(src, dst, send, recv, **to):
    return pltpu.make_async_remote_copy(
        src_ref=src, dst_ref=dst, send_sem=send, recv_sem=recv, device_id=to, device_id_type=MESH
    )


class Where:
    def __init__(self):
        self.sp = lax.axis_index("sp")
        self.x = lax.axis_index("tp")
        self.core = lax.rem(self.sp, 2)
        self.other = self.sp + 1 - 2 * self.core
        self.chip = self.sp // 2
        self.y = lax.rem(self.chip, 4)
        self.z = self.chip // 4
        self.zl = lax.rem(self.z, 2)
        self.late = self.z // 2

    def chip_behind(self, dy, dz):
        return lax.rem(self.z + 4 - dz, 4) * 4 + lax.rem(self.y + 4 - dy, 4)

    def step(self, axis, forward):
        d = 3 if forward else 1
        return (self.chip_behind(d, 0) if axis == "y" else self.chip_behind(0, d)) * 2 + self.core

    def pair(self):
        return ((self.z + 1 - 2 * self.zl) * 4 + self.y) * 2 + self.core

    def opposite(self):
        return ((3 - self.z) * 4 + self.y) * 2 + self.core

    def half_chip(self, dy, zo):
        zl = self.zl + zo - 2 * zo * self.zl
        return zl * 4 + lax.rem(self.y + 4 - dy, 4)


class Gather:
    def __init__(self, at, buf, first, send, recv, drecv):
        self.at, self.buf, self.send, self.recv, self.drecv = at, buf, send, recv, drecv
        self.axes = {"f": first, "g": "z" if first == "y" else "y"}
        self.half = buf.shape[1] // 2

    def slot(self, df, dg):
        dy, dz = (df, dg) if self.axes["f"] == "y" else (dg, df)
        return self.at.chip_behind(dy, dz) * 2 + self.at.core

    def copy(self, ident, slot, half, to):
        ref = self.buf.at[slot]
        if half is not None:
            ref = self.buf.at[slot, pl.ds(half * self.half, self.half)]
        return remote(ref, ref, self.send, self.recv.at[ident], sp=to)

    def out(self, ident, df, dg, half, axis, forward):
        self.copy(ident, self.slot(df, dg), half, self.at.step(self.axes[axis], forward)).start()

    def into(self, ident, df, dg):
        self.copy(ident, self.slot(df, dg), None, self.at.other).wait_recv()

    def across(self, df, dg, far=0):
        ref = self.buf.at[self.slot(df, dg)]
        remote(ref, ref, self.send, self.drecv.at[far], sp=self.at.other).start()

    def start_along(self, axis, forward):
        self.out((0 if axis == "f" else 3) + (not forward), 0, 0, None, axis, forward)

    def along_second(self, j):
        self.second_step(j, True)
        self.second_step(j, False)
        self.across(FIRST[j], 0)

    def second_step(self, j, forward):
        self.out((3 if forward else 4) + 3 * j, FIRST[j], 0, None, "g", forward)

    def got_first(self):
        self.into(0, 1, 0)
        self.into(1, 3, 0)

    def first_step(self, forward):
        if forward:
            self.out(2, 1, 0, 0, "f", True)
        else:
            self.out(2, 3, 0, 1, "f", False)

    def got_second(self, j, uneven=False):
        self.into(3 + 3 * j, FIRST[j], 1)
        self.into(4 + 3 * j, FIRST[j], 3)

        def pass_on(cut):
            for df, dg, start, stop in ((FIRST[j], 1, 0, cut), (FIRST[j], 3, cut, 2 * self.half)):
                ref = self.buf.at[self.slot(df, dg), pl.ds(start, stop - start)]
                to = self.at.step(self.axes["g"], dg == 1)
                remote(ref, ref, self.send, self.recv.at[5 + 3 * j], sp=to).start()

        if uneven:
            for zl, cut in ((0, self.half // 2), (1, 3 * self.half // 2)):
                pl.when(self.at.zl == zl)(functools.partial(pass_on, cut))
        else:
            pass_on(self.half)
        self.across(FIRST[j], 1)
        self.across(FIRST[j], 3)

    def got_opposite(self):
        self.into(2, 2, 0)
        self.along_second(3)

    def got_far(self, j):
        self.into(5 + 3 * j, FIRST[j], 2)
        self.across(FIRST[j], 2, 1)

    def from_other(self, far):
        ref = self.buf.at[pl.ds(0, 4 if far else 12)]
        remote(ref, ref, self.send, self.drecv.at[far], sp=self.at.other).wait_recv()

    def drain(self):
        ref = self.buf.at[pl.ds(0, 31)]
        remote(ref, ref, self.send, self.drecv.at[0], sp=self.at.other).wait_send()


class HalfGather:
    def __init__(self, at, buf, send, recv, drecv):
        self.at, self.buf, self.send, self.recv, self.drecv = at, buf, send, recv, drecv
        self.half = buf.shape[1] // 2

    def slot(self, dy, zo):
        return self.at.half_chip(dy, zo) * 2 + self.at.core

    def copy(self, ident, dy, zo, half, to):
        ref = self.buf.at[self.slot(dy, zo)]
        if half is not None:
            ref = self.buf.at[self.slot(dy, zo), pl.ds(half * self.half, self.half)]
        return remote(ref, ref, self.send, self.recv.at[ident], sp=to)

    def out(self, ident, dy, zo, half, to):
        self.copy(ident, dy, zo, half, to).start()

    def into(self, ident, dy, zo):
        self.copy(ident, dy, zo, None, self.at.other).wait_recv()

    def over(self, t, slot):
        ref = self.buf.at[slot]
        return remote(ref, ref, self.send, self.drecv.at[t], sp=self.at.other)

    def across(self, dy, zo):
        self.over(HALF_STEP_OF[dy, zo], self.slot(dy, zo)).start()

    def both_from_other(self, t):
        ref = self.buf.at[pl.ds(0, 2)]
        remote(ref, ref, self.send, self.drecv.at[t], sp=self.at.other).wait_recv()

    def ring_start(self, ident, zo):
        self.out(ident, 0, zo, None, self.at.step("y", True))
        self.out(ident + 1, 0, zo, None, self.at.step("y", False))

    def ring_middle(self, ident, zo, after=lambda dy: None):
        self.into(ident, 1, zo)
        self.out(ident + 2, 1, zo, 0, self.at.step("y", True))
        after(1)
        self.across(1, zo)
        self.into(ident + 1, 3, zo)
        self.out(ident + 2, 3, zo, 1, self.at.step("y", False))
        after(3)
        self.across(3, zo)

    def ring_end(self, ident, zo, after=lambda dy: None):
        self.into(ident + 2, 2, zo)
        after(2)
        self.across(2, zo)

    def drain(self):
        ref = self.buf.at[pl.ds(0, 15)]
        remote(ref, ref, self.send, self.recv.at[0], sp=self.at.other).wait_send()


def kernel(
    lam_in, sub_in, norm_in, conv_g_in, conv_u_in,
    q_in, k_in, v_in, wg_in, wu_in, wo_in, wd_in, res_in,
    out,
    lam, sub_gain, norm_gain, conv_g, conv_u, q_raw, k_raw, v_raw, q, kbuf, vbuf, wg, wu, wo, wd, res,
    m_s, l_s, acc, a_far, stat, stat_far, n_all, mid, hn, pre, hid, part, relay, parts, ended,
    lsem, send, krecv, kdrecv, wrecv, drecv, orecv, xrecv, precv,
):
    at = Where()
    x, sp, core, other = at.x, at.sp, at.core, at.other
    rows = q.shape[1]
    own = rows // 4
    late = at.late == 1
    early = at.late == 0
    mine = at.half_chip(0, 0)

    barrier = pltpu.get_barrier_semaphore()
    after, before = lax.rem(sp + 1, 32), lax.rem(sp + 31, 32)
    for to in (other, at.step("y", True), at.step("y", False), at.step("z", True), at.step("z", False)):
        pl.semaphore_signal(barrier, inc=1, device_id={"sp": to}, device_id_type=MESH)
    for to in (after, before):
        for x_to in range(4):
            pl.semaphore_signal(barrier, inc=1, device_id={"sp": to, "tp": x_to}, device_id_type=MESH)
    xs = [lax.rem(x + d, 4) for d in range(4)]
    for to in xs[1:]:
        pl.semaphore_signal(barrier, inc=1, device_id={"tp": to}, device_id_type=MESH)

    loads = [
        pltpu.make_async_copy(src, dst, lsem.at[i])
        for i, (src, dst) in enumerate(
            (
                (k_in, k_raw), (v_in, v_raw), (q_in, q_raw), (wo_in, wo.at[x]), (wg_in, wg.at[sp]), (wu_in, wu.at[sp]),
                (wd_in, wd), (res_in, res.at[pl.ds(16, rows)]), (lam_in, lam), (sub_in, sub_gain),
                (norm_in, norm_gain), (conv_g_in, conv_g), (conv_u_in, conv_u),
            )
        )
    ]
    for load in loads[:3]:
        load.start()
    loads[0].wait()
    kbuf[mine * 2 + core] = k_raw[...].reshape(kbuf.shape[1:])
    for load in loads[3:6] + loads[7:]:
        load.start()
    with jax.named_scope("barrier"):
        pl.semaphore_wait(barrier, 16)

    keys = HalfGather(at, kbuf, send.at[0], krecv.at[0], kdrecv)
    vals = HalfGather(at, vbuf, send.at[1], krecv.at[1], kdrecv)
    gate = Gather(at, wg, "y", send.at[2], wrecv.at[0], drecv.at[0])
    up = Gather(at, wu, "z", send.at[3], wrecv.at[1], drecv.at[1])

    def key_on(dy):
        keys.out(3 + FIRST.index(dy), dy, 0, None, at.pair())

    def q_copy():
        return remote(q.at[0], q.at[1], send.at[9], orecv.at[0], sp=at.opposite())

    keys.ring_start(0, 0)
    loads[1].wait()
    vbuf[mine * 2 + core] = v_raw[...].reshape(vbuf.shape[1:])
    vals.out(0, 0, 0, None, at.pair())
    key_on(0)
    vals.ring_start(1, 0)
    keys.across(0, 0)
    vals.across(0, 0)
    loads[2].wait()
    q[0] = q_raw[...].reshape(q.shape[1:])

    @pl.when(late)
    def _():
        q_copy().start()

    def weights_along_z(forward):
        gate.start_along("g", forward)
        up.start_along("f", forward)

    loads[4].wait()
    loads[5].wait()
    for forward in (True, False):
        pl.when(at.zl == int(forward))(functools.partial(weights_along_z, forward))

    def weights_start():
        for forward in (True, False):
            up.start_along("g", forward)
            pl.when(at.zl == int(not forward))(functools.partial(weights_along_z, forward))
        gate.across(0, 0)
        up.across(0, 0)

    wo_half = wo.shape[1] // 2
    wo_quarter = wo_half // 2

    def wo_copy(ident, slot, start, size, to):
        ref = wo.at[slot, pl.ds(core * wo_half + start, size)]
        return remote(ref, ref, send.at[4], xrecv.at[ident], tp=to)

    def wo_over(slot):
        ref = wo.at[slot, pl.ds(core * wo_half, wo_half)]
        return remote(ref, ref, send.at[4], xrecv.at[3], sp=other)

    def res_copy(to):
        return remote(res.at[pl.ds(rows, 16)], res.at[pl.ds(0, 16)], send.at[6], xrecv.at[8], sp=to)

    def n_halo_copy(slot, to, x_to):
        return remote(
            n_all.at[slot, pl.ds(rows, 16)], n_all.at[slot, pl.ds(0, 16)], send.at[7], xrecv.at[9], sp=to, tp=x_to
        )

    loads[7].wait()
    loads[6].start()

    @pl.when(sp < 31)
    def _():
        res_copy(after).start()

    @pl.when(sp == 0)
    def _():
        res[:16, :] = jnp.zeros((16, res.shape[1]), BF16)
        n_all[:, :16, :] = jnp.zeros((4, 16, n_all.shape[2]), BF16)

    loads[3].wait()
    wo_copy(0, x, 0, wo_half, xs[1]).start()
    wo_copy(1, x, 0, wo_half, xs[3]).start()

    def wo_middle():
        wo_copy(0, xs[3], 0, wo_half, xs[1]).wait_recv()
        wo_copy(2, xs[3], 0, wo_quarter, xs[1]).start()
        wo_over(xs[3]).start()
        wo_copy(1, xs[1], 0, wo_half, xs[3]).wait_recv()
        wo_copy(2, xs[1], wo_quarter, wo_quarter, xs[3]).start()
        wo_over(xs[1]).start()

    def wo_end():
        wo_copy(2, xs[2], 0, wo_half, xs[1]).wait_recv()
        wo_over(xs[2]).start()

    def wo_wait():
        ref = wo.at[pl.ds(0, 3), pl.ds(0, wo_half)]
        remote(ref, ref, send.at[4], xrecv.at[3], sp=other).wait_recv()

    scale = 1.0 / math.sqrt(128.0) / math.log(2.0)

    def block(who, chip, masked):
        for j in range(4):
            h = j // 2
            kj = kbuf[pl.ds(chip * 2, 2), :, 128 * j : 128 * j + 128].reshape(2 * rows, 128)
            vj = vbuf[pl.ds(chip * 2, 2), :, 256 * h : 256 * h + 256].reshape(2 * rows, 256)
            s = lax.dot_general(
                q[who, :, 128 * j : 128 * j + 128], kj, (((1,), (1,)), ((), ())), preferred_element_type=F32
            )
            s = s * scale
            if masked:
                q_pos = lax.broadcasted_iota(jnp.int32, s.shape, 0) + core * rows
                s = jnp.where(lax.broadcasted_iota(jnp.int32, s.shape, 1) <= q_pos, s, -1e30)
            top = jnp.max(s, axis=1, keepdims=True)
            if masked:
                m_new = top
            else:
                m_old = m_s[4 * who + j][:, :1]
                m_new = jnp.maximum(m_old, top)
                alpha = jnp.exp2(m_old - m_new)
            p = jnp.exp2(s - m_new)
            part_sum = p[:, :128]
            for i in range(1, 2 * rows // 128):
                part_sum = part_sum + p[:, 128 * i : 128 * i + 128]
            pv = jnp.dot(p.astype(BF16), vj, preferred_element_type=F32)
            m_s[4 * who + j] = jnp.broadcast_to(m_new, (rows, 128))
            if masked:
                l_s[4 * who + j] = part_sum
                acc[4 * who + j] = pv
            else:
                l_s[4 * who + j] = l_s[4 * who + j] * alpha + part_sum
                acc[4 * who + j] = acc[4 * who + j] * alpha + pv

    @pl.when(early)
    def _():
        m_s[4:] = jnp.full((4, rows, 128), -1e30, F32)
        l_s[4:] = jnp.zeros((4, rows, 128), F32)
        acc[4:] = jnp.zeros((4, *acc.shape[1:]), F32)

    with jax.named_scope("own_wait"):
        keys.both_from_other(0)
    with jax.named_scope("own_block"):
        block(0, mine, True)

    def handler_0():
        keys.ring_middle(0, 0, key_on)
        vals.into(0, 0, 1)
        vals.ring_start(4, 1)
        for forward in (True, False):
            gate.start_along("f", forward)
        vals.across(0, 1)
        vals.ring_middle(1, 0)
        keys.into(3, 0, 1)
        keys.across(0, 1)

        @pl.when(early)
        def _():
            q_copy().wait_recv()

    def handler_2():
        keys.ring_end(0, 0, key_on)

    def gate_along_z(forward):
        gate.second_step(1, forward)
        gate.second_step(2, forward)

    def handler_4():
        vals.ring_middle(4, 1)
        for ident, dy in ((4, 1), (5, 3)):
            keys.into(ident, dy, 1)
            keys.across(dy, 1)

    def handler_5():
        gate.got_first()
        for forward in (True, False):
            pl.when(at.zl == int(forward))(functools.partial(gate_along_z, forward))
        weights_start()
        wo_middle()
        vals.ring_end(1, 0)

    def handler_6():
        vals.ring_end(4, 1)
        keys.into(6, 2, 1)
        keys.across(2, 1)

    def step(t, carry):
        for when, handler in (
            (0, handler_0), (2, handler_2), (4, handler_4), (5, handler_5), (6, handler_6)
        ):

            @pl.when(t == when)
            def _():
                with jax.named_scope(handler.__name__):
                    handler()

        dy, zo = (pick(t, [d[i] for d in HALF_ORDER]) for i in (0, 1))
        chip = at.half_chip(dy, zo)

        @pl.when(t > 0)
        def _():
            with jax.named_scope("d2d_wait"):
                keys.both_from_other(t)

        @pl.when(early)
        def _():
            with jax.named_scope("far_block"):
                block(1, chip, False)

        @pl.when(chip < mine)
        def _():
            with jax.named_scope("block"):
                block(0, chip, False)

        return carry

    lax.fori_loop(0, 8, step, 0)

    def stat_copy():
        return remote(stat, stat_far, send.at[10], orecv.at[1], sp=at.opposite())

    def a_copy(h):
        return remote(a_far.at[h], a_far.at[h], send.at[11], orecv.at[2 + h], sp=at.opposite())

    loads[8].wait()
    loads[9].wait()
    lanes = lax.broadcasted_iota(jnp.int32, (rows, 128), 1)
    base = 4 - 4 * at.late
    stats = jnp.zeros((rows, 128), F32)
    for j in range(4):
        total = jnp.sum(l_s[base + j], axis=1, keepdims=True)
        stats = jnp.where(lanes == j, m_s[base + j], jnp.where(lanes == 4 + j, total, stats))
    stat[...] = stats.T[:8]
    stat_copy().start()

    with jax.named_scope("w_first"):
        for forward in (True, False):
            gate.first_step(forward)
        up.got_first()
        for forward in (True, False):
            up.first_step(forward)
            pl.when(at.zl == int(not forward))(functools.partial(gate_along_z, forward))
        for j in (1, 2):
            up.along_second(j)
            gate.across(FIRST[j], 0)

    with jax.named_scope("stat_wait"):
        stat_copy().wait_recv()

    with jax.named_scope("blend"):
        here = jnp.concatenate([stat[...], jnp.zeros((120, rows), F32)], axis=0).T
        there = jnp.concatenate([stat_far[...], jnp.zeros((120, rows), F32)], axis=0).T
        for h in range(2):
            shares = []
            for j in (2 * h, 2 * h + 1):
                m_here, m_there = here[:, j : j + 1], there[:, j : j + 1]
                top = jnp.maximum(m_here, m_there)
                e_here, e_there = jnp.exp2(m_here - top), jnp.exp2(m_there - top)
                total = here[:, 4 + j : 5 + j] * e_here + there[:, 4 + j : 5 + j] * e_there
                shares.append(acc[base + j] * (e_here / total))
            a = shares[0] - lam[h] * shares[1]

            @pl.when(early)
            def _():
                a_far[h] = a.astype(BF16)
                a_copy(h).start()

            @pl.when(late)
            def _():
                acc[2 * h] = a

    with jax.named_scope("w_second"):
        gate.got_second(0)
        up.got_second(0)
        gate.got_opposite()
        up.got_opposite()

    for h in range(2):

        @pl.when(late)
        def _():
            with jax.named_scope("a_wait"):
                a_copy(h).wait_recv()
            acc[2 * h] = acc[2 * h] + a_far[h].astype(F32)

        @pl.when(early)
        def _():
            mixed = []
            for j in (2 * h, 2 * h + 1):
                mixed.append(acc[j] / jnp.sum(l_s[j], axis=1, keepdims=True))
            acc[2 * h] = mixed[0] - lam[h] * mixed[1]

        a = acc[2 * h]
        square = jnp.mean(a * a, axis=1, keepdims=True)
        n = a * lax.rsqrt(square + EPS) * sub_gain[...] * (1.0 - LAMBDA_INIT)
        n_all[x, 16:, 256 * h : 256 * h + 256] = n.astype(BF16)

    def n_copy(ident, slot, start, size, to):
        ref = n_all.at[slot, pl.ds(16 + start, size)]
        return remote(ref, ref, send.at[5], xrecv.at[4 + ident], tp=to)

    @pl.when(sp < 31)
    def _():
        for x_to in range(4):
            n_halo_copy(x, after, x_to).start()

    n_copy(0, x, 0, rows, xs[1]).start()
    n_copy(1, x, 0, rows, xs[3]).start()

    with jax.named_scope("wo_end"):
        wo_end()
    with jax.named_scope("w_third"):
        for j in (1, 2):
            gate.got_second(j, uneven=True)
            up.got_second(j)
    with jax.named_scope("n_middle"):
        n_copy(0, xs[3], 0, rows, xs[1]).wait_recv()
        n_copy(2, xs[3], 0, rows // 2, xs[1]).start()
        n_copy(1, xs[1], 0, rows, xs[3]).wait_recv()
        n_copy(2, xs[1], rows // 2, rows // 2, xs[3]).start()

    with jax.named_scope("w_fourth"):
        up.got_second(3)
        gate.got_second(3)

    @pl.when(sp > 0)
    def _():
        with jax.named_scope("halo_wait"):
            res_copy(before).wait_recv()
            ref = n_all.at[pl.ds(0, 4), pl.ds(0, 16)]
            remote(ref, ref, send.at[7], xrecv.at[9], sp=before).wait_recv()

    def project(slots, first):
        def body(i, carry):
            cols = pl.ds(pl.multiple_of(i * 256, 256), 256)
            sums = res[:, cols].astype(F32) if first else mid[:, cols]
            for slot in slots:
                sums = sums + jnp.dot(n_all[slot], wo[slot, :, cols], preferred_element_type=F32)
            mid[:, cols] = sums
            return carry

        lax.fori_loop(0, mid.shape[1] // 256, body, 0, unroll=2)

    with jax.named_scope("wo_wait"):
        wo_wait()
    with jax.named_scope("project"):
        project((x, xs[1], xs[3]), True)
    with jax.named_scope("n_wait"):
        n_copy(2, xs[2], 0, rows, xs[1]).wait_recv()
    with jax.named_scope("project_last"):
        project((xs[2],), False)
    for load in loads[10:]:
        load.wait()
    with jax.named_scope("norm"):
        middle = mid[...]
        square = jnp.mean(middle * middle, axis=1, keepdims=True)
        hn[...] = (middle * lax.rsqrt(square + EPS) * norm_gain[...]).astype(BF16)
    feats = hn.shape[1]
    units = wg.shape[2]
    row, place = feats // 4, feats // 16

    def gate_part(dz, cols):
        z = lax.rem(at.z + dz, 4)
        return jnp.dot(
            hn[:, pl.ds(pl.multiple_of(z * row, row), row)], wg[pl.ds(z * 8, 8), :, cols].reshape(row, -1),
            preferred_element_type=F32,
        )

    def up_part(dy, cols):
        y = lax.rem(at.y + dy, 4)
        left = [hn[:, pl.ds(pl.multiple_of(z * row + y * place, place), place)] for z in range(4)]
        right = [wu[pl.ds(z * 8 + y * 2, 2), :, cols].reshape(place, -1) for z in range(4)]
        return jnp.dot(
            jnp.concatenate(left, axis=1), jnp.concatenate(right, axis=0), preferred_element_type=F32
        )

    def mix(g, taps):
        return taps[0:1] * pltpu.roll(g, 2, 0) + taps[1:2] * pltpu.roll(g, 1, 0) + taps[2:3] * g

    def feed_most(at_col, width):
        cols = pl.ds(at_col, width)
        for i, part_of in enumerate((gate_part, up_part)):
            pre[i, :, cols] = part_of(0, cols) + part_of(1, cols) + part_of(3, cols)

    def feed_last(at_col, width):
        cols = pl.ds(at_col, width)
        mixed = []
        for i, (part_of, taps) in enumerate(((gate_part, conv_g), (up_part, conv_u))):
            g = (pre[i, :, cols] + part_of(2, cols)).astype(BF16).astype(F32)
            mixed.append(mix(g, taps[:, cols])[16:])
        gc, uc = mixed
        hid[:, cols] = (gc * (1.0 / (1.0 + jnp.exp(-gc))) * uc).astype(BF16)

    def feed(body):
        for start in range(0, units, 256):
            body(start, min(256, units - start))

    with jax.named_scope("w_rest"):
        gate.from_other(0)
        up.from_other(0)
    with jax.named_scope("feed_most"):
        feed(feed_most)
    with jax.named_scope("w_fifth"):
        for j in range(4):
            gate.got_far(j)
            up.got_far(j)
    with jax.named_scope("w_over"):
        gate.from_other(1)
        up.from_other(1)
        loads[6].wait()
    with jax.named_scope("feed"):
        feed(feed_last)

    chunks = part.shape[2] // 512
    side = own // 2

    def cols_of(i):
        return pl.ds(pl.multiple_of(i * 512, 512), 512)

    def relay_copy(s, i, to):
        return remote(
            part.at[xs[2], pl.ds(s * side, side), cols_of(i)], relay.at[s, :, cols_of(i)],
            send.at[8], precv.at[0, i], tp=to,
        )

    def part_copy(s, i, to):
        return remote(
            part.at[to, :, cols_of(i)], parts.at[s, :, cols_of(i)], send.at[8], precv.at[1, i], tp=to
        )

    def arrived(buf, which, i):
        ref = buf.at[:, :, cols_of(i)]
        remote(ref, ref, send.at[8], precv.at[which, i], tp=xs[1]).wait_recv()

    def lower(i, carry):
        cols = cols_of(i)
        full = jnp.dot(hid[...], wd[:, cols], preferred_element_type=F32).astype(BF16)
        part[:, :, cols] = full.reshape(4, own, 512)
        relay_copy(0, i, xs[1]).start()
        relay_copy(1, i, xs[3]).start()
        return carry

    with jax.named_scope("lower"):
        lax.fori_loop(0, chunks, lower, 0, unroll=True)

    def pass_on(i, carry):
        cols = cols_of(i)
        arrived(relay, 0, i)
        for s, to in ((0, xs[1]), (1, xs[3])):
            half = pl.ds(s * side, side)
            both = part[to, half, cols].astype(F32) + relay[s, :, cols].astype(F32)
            part[to, half, cols] = both.astype(BF16)
            part_copy(s, i, to).start()
        return carry

    def sent(ref, which):
        remote(ref, ref, send.at[which], xrecv.at[0], sp=other).wait_send()

    with jax.named_scope("drain"):
        for gather in (keys, vals, gate, up):
            gather.drain()
        sent(wo.at[pl.ds(0, 3)], 4)
        sent(n_all.at[pl.ds(0, 3), pl.ds(0, rows)], 5)
        stat_copy().wait_send()

        @pl.when(sp < 31)
        def _():
            sent(hn.at[pl.ds(0, 16)], 6)
            sent(n_all.at[pl.ds(0, 4), pl.ds(0, 16)], 7)

        @pl.when(late)
        def _():
            q_copy().wait_send()

        @pl.when(early)
        def _():
            sent(a_far, 11)

    with jax.named_scope("pass_on"):
        lax.fori_loop(0, chunks, pass_on, 0)

    def finish(i, carry):
        cols = cols_of(i)
        arrived(parts, 1, i)
        sums = parts[0, :, cols].astype(F32) + parts[1, :, cols].astype(F32) + part[x, :, cols].astype(F32)
        middle = mid[pl.ds(pl.multiple_of(16 + x * own, 16), own), cols]
        ended[:, cols] = (middle + sums).astype(BF16)
        pltpu.make_async_copy(ended.at[:, cols], out.at[:, cols], lsem.at[i]).start()
        return carry

    with jax.named_scope("finish"):
        lax.fori_loop(0, chunks, finish, 0)

    sent(hn.at[pl.ds(0, 3 * own)], 8)
    for i in range(chunks):
        pltpu.make_async_copy(ended.at[:, cols_of(i)], out.at[:, cols_of(i)], lsem.at[i]).wait()


def local(
    residual, queries, key_rows, values, lambda_head, sub_gain, w_out, norm_gain, w_gate, w_up, conv_gate, conv_up,
    w_down,
):
    rows = queries.shape[0]
    d = residual.shape[1]
    own = rows // 4
    heads_wide = queries.shape[1] * values.shape[2]
    units = w_gate.shape[1]
    maps = queries.shape[1] * 2
    places = 32
    hbm = pl.BlockSpec(memory_space=pl.ANY)
    dma = pltpu.SemaphoreType.DMA
    call = pl.pallas_call(
        kernel,
        out_shape=jax.ShapeDtypeStruct((own, d), BF16),
        in_specs=[hbm] * 13,
        out_specs=hbm,
        scratch_shapes=[
            pltpu.SMEM(lambda_head.shape, F32),
            pltpu.VMEM((1, *sub_gain.shape), F32),
            pltpu.VMEM((1, d), F32),
            pltpu.VMEM(conv_gate.shape, F32),
            pltpu.VMEM(conv_up.shape, F32),
            pltpu.VMEM(queries.shape, BF16),
            pltpu.VMEM(key_rows.shape, BF16),
            pltpu.VMEM(values.shape, BF16),
            pltpu.VMEM((2, rows, 512), BF16),
            pltpu.VMEM((places // 2, rows, 512), BF16),
            pltpu.VMEM((places // 2, rows, 512), BF16),
            pltpu.VMEM((places, w_gate.shape[0], units), BF16),
            pltpu.VMEM((places, w_gate.shape[0], units), BF16),
            pltpu.VMEM((4, *w_out.shape), BF16),
            pltpu.VMEM(w_down.shape, BF16),
            pltpu.VMEM((rows + 16, d), BF16),
            pltpu.VMEM((2 * maps, rows, 128), F32),
            pltpu.VMEM((2 * maps, rows, 128), F32),
            pltpu.VMEM((2 * maps, rows, values.shape[2]), F32),
            pltpu.VMEM((2, rows, values.shape[2]), BF16),
            pltpu.VMEM((8, rows), F32),
            pltpu.VMEM((8, rows), F32),
            pltpu.VMEM((4, rows + 16, heads_wide), BF16),
            pltpu.VMEM((rows + 16, d), F32),
            pltpu.VMEM((rows + 16, d), BF16),
            pltpu.VMEM((2, rows + 16, units), F32),
            pltpu.VMEM((rows, units), BF16),
            pltpu.VMEM((4, own, d), BF16),
            pltpu.VMEM((2, own // 2, d), BF16),
            pltpu.VMEM((2, own, d), BF16),
            pltpu.VMEM((own, d), BF16),
            dma((13,)), dma((12,)), dma((2, 7)), dma((8,)), dma((2, 15)), dma((2, 2)), dma((4,)), dma((10,)),
            dma((2, d // 512)),
        ],
        compiler_params=pltpu.CompilerParams(
            collective_id=0, has_side_effects=True, vmem_limit_bytes=67043328
        ),
    )
    return call(
        lambda_head, sub_gain[None], norm_gain[None], conv_gate, conv_up,
        queries, key_rows, values,
        w_gate, w_up, w_out, w_down, residual,
    )


def solution(mesh):
    placed = (
        P("sp", None),
        P("sp", "tp", None, None),
        P("sp", "tp", None, None),
        P("sp", "tp", None),
        P("tp"),
        P(),
        P("tp", None),
        P(),
        P("sp", "tp"),
        P("sp", "tp"),
        P(None, "tp"),
        P(None, "tp"),
        P("tp", None),
    )
    return jax.shard_map(
        local, mesh=mesh, in_specs=placed, out_specs=P(("sp", "tp"), None), check_vma=False
    )
```

```python
import functools
import math

import jax
import jax.numpy as jnp
from jax import lax
from jax.experimental import pallas as pl
from jax.experimental.pallas import tpu as pltpu
from jax.sharding import PartitionSpec as P

EPS = 1e-06
LAMBDA_INIT = 0.8 - 0.6 * math.exp(-0.3)
BF16, F32 = jnp.bfloat16, jnp.float32
MESH = pl.DeviceIdType.MESH

ORDER = (
    (0, 0),
    (1, 0), (3, 0), (0, 1), (0, 3),
    (1, 1), (1, 3), (3, 1), (3, 3),
    (2, 0), (0, 2),
    (2, 1), (2, 3), (1, 2), (3, 2),
    (2, 2),
)
STEP_OF = {d: t for t, d in enumerate(ORDER)}
FIRST = (0, 1, 3, 2)
HALF_ORDER = ((0, 0), (1, 0), (3, 0), (0, 1), (1, 1), (3, 1), (2, 0), (2, 1))
HALF_STEP_OF = {d: t for t, d in enumerate(HALF_ORDER)}


def pick(t, values):
    return sum(jnp.where(t == i, v, 0) for i, v in enumerate(values) if v)


def remote(src, dst, send, recv, **to):
    return pltpu.make_async_remote_copy(
        src_ref=src, dst_ref=dst, send_sem=send, recv_sem=recv, device_id=to, device_id_type=MESH
    )


class Where:
    def __init__(self):
        self.sp = lax.axis_index("sp")
        self.x = lax.axis_index("tp")
        self.core = lax.rem(self.sp, 2)
        self.other = self.sp + 1 - 2 * self.core
        self.chip = self.sp // 2
        self.y = lax.rem(self.chip, 4)
        self.z = self.chip // 4
        self.zl = lax.rem(self.z, 2)
        self.late = self.z // 2

    def chip_behind(self, dy, dz):
        return lax.rem(self.z + 4 - dz, 4) * 4 + lax.rem(self.y + 4 - dy, 4)

    def step(self, axis, forward):
        d = 3 if forward else 1
        return (self.chip_behind(d, 0) if axis == "y" else self.chip_behind(0, d)) * 2 + self.core

    def pair(self):
        return ((self.z + 1 - 2 * self.zl) * 4 + self.y) * 2 + self.core

    def opposite(self):
        return ((3 - self.z) * 4 + self.y) * 2 + self.core

    def half_chip(self, dy, zo):
        zl = self.zl + zo - 2 * zo * self.zl
        return zl * 4 + lax.rem(self.y + 4 - dy, 4)


class Gather:
    def __init__(self, at, buf, first, send, recv, drecv):
        self.at, self.buf, self.send, self.recv, self.drecv = at, buf, send, recv, drecv
        self.axes = {"f": first, "g": "z" if first == "y" else "y"}
        self.half = buf.shape[1] // 2

    def slot(self, df, dg):
        dy, dz = (df, dg) if self.axes["f"] == "y" else (dg, df)
        return self.at.chip_behind(dy, dz) * 2 + self.at.core

    def copy(self, ident, slot, half, to):
        ref = self.buf.at[slot]
        if half is not None:
            ref = self.buf.at[slot, pl.ds(half * self.half, self.half)]
        return remote(ref, ref, self.send, self.recv.at[ident], sp=to)

    def out(self, ident, df, dg, half, axis, forward):
        self.copy(ident, self.slot(df, dg), half, self.at.step(self.axes[axis], forward)).start()

    def into(self, ident, df, dg):
        self.copy(ident, self.slot(df, dg), None, self.at.other).wait_recv()

    def across(self, df, dg, far=0):
        ref = self.buf.at[self.slot(df, dg)]
        remote(ref, ref, self.send, self.drecv.at[far], sp=self.at.other).start()

    def start_along(self, axis, forward):
        self.out((0 if axis == "f" else 3) + (not forward), 0, 0, None, axis, forward)

    def along_second(self, j):
        self.second_step(j, True)
        self.second_step(j, False)
        self.across(FIRST[j], 0)

    def second_step(self, j, forward):
        self.out((3 if forward else 4) + 3 * j, FIRST[j], 0, None, "g", forward)

    def got_first(self):
        self.into(0, 1, 0)
        self.into(1, 3, 0)

    def first_step(self, forward):
        if forward:
            self.out(2, 1, 0, 0, "f", True)
        else:
            self.out(2, 3, 0, 1, "f", False)

    def got_second(self, j, uneven=False):
        self.into(3 + 3 * j, FIRST[j], 1)
        self.into(4 + 3 * j, FIRST[j], 3)

        def pass_on(cut):
            for df, dg, start, stop in ((FIRST[j], 1, 0, cut), (FIRST[j], 3, cut, 2 * self.half)):
                ref = self.buf.at[self.slot(df, dg), pl.ds(start, stop - start)]
                to = self.at.step(self.axes["g"], dg == 1)
                remote(ref, ref, self.send, self.recv.at[5 + 3 * j], sp=to).start()

        if uneven:
            for zl, cut in ((0, self.half // 2), (1, 3 * self.half // 2)):
                pl.when(self.at.zl == zl)(functools.partial(pass_on, cut))
        else:
            pass_on(self.half)
        self.across(FIRST[j], 1)
        self.across(FIRST[j], 3)

    def got_opposite(self):
        self.into(2, 2, 0)
        self.along_second(3)

    def got_far(self, j):
        self.into(5 + 3 * j, FIRST[j], 2)
        self.across(FIRST[j], 2, 1)

    def from_other(self, far):
        ref = self.buf.at[pl.ds(0, 4 if far else 12)]
        remote(ref, ref, self.send, self.drecv.at[far], sp=self.at.other).wait_recv()

    def drain(self):
        ref = self.buf.at[pl.ds(0, 31)]
        remote(ref, ref, self.send, self.drecv.at[0], sp=self.at.other).wait_send()


class HalfGather:
    def __init__(self, at, buf, send, recv, drecv):
        self.at, self.buf, self.send, self.recv, self.drecv = at, buf, send, recv, drecv
        self.half = buf.shape[1] // 2

    def slot(self, dy, zo):
        return self.at.half_chip(dy, zo) * 2 + self.at.core

    def copy(self, ident, dy, zo, half, to):
        ref = self.buf.at[self.slot(dy, zo)]
        if half is not None:
            ref = self.buf.at[self.slot(dy, zo), pl.ds(half * self.half, self.half)]
        return remote(ref, ref, self.send, self.recv.at[ident], sp=to)

    def out(self, ident, dy, zo, half, to):
        self.copy(ident, dy, zo, half, to).start()

    def into(self, ident, dy, zo):
        self.copy(ident, dy, zo, None, self.at.other).wait_recv()

    def over(self, t, slot):
        ref = self.buf.at[slot]
        return remote(ref, ref, self.send, self.drecv.at[t], sp=self.at.other)

    def across(self, dy, zo):
        self.over(HALF_STEP_OF[dy, zo], self.slot(dy, zo)).start()

    def both_from_other(self, t):
        ref = self.buf.at[pl.ds(0, 2)]
        remote(ref, ref, self.send, self.drecv.at[t], sp=self.at.other).wait_recv()

    def ring_start(self, ident, zo):
        self.out(ident, 0, zo, None, self.at.step("y", True))
        self.out(ident + 1, 0, zo, None, self.at.step("y", False))

    def ring_middle(self, ident, zo, after=lambda dy: None):
        self.into(ident, 1, zo)
        self.out(ident + 2, 1, zo, 0, self.at.step("y", True))
        after(1)
        self.across(1, zo)
        self.into(ident + 1, 3, zo)
        self.out(ident + 2, 3, zo, 1, self.at.step("y", False))
        after(3)
        self.across(3, zo)

    def ring_end(self, ident, zo, after=lambda dy: None):
        self.into(ident + 2, 2, zo)
        after(2)
        self.across(2, zo)

    def drain(self):
        ref = self.buf.at[pl.ds(0, 15)]
        remote(ref, ref, self.send, self.recv.at[0], sp=self.at.other).wait_send()


def kernel(
    lam_in, sub_in, norm_in, conv_g_in, conv_u_in,
    q_in, k_in, v_in, wg_in, wu_in, wo_in, wd_in, res_in,
    out,
    lam, sub_gain, norm_gain, conv_g, conv_u, q_raw, k_raw, v_raw, q, kbuf, vbuf, wg, wu, wo, wd, res,
    m_s, l_s, acc, a_far, stat, stat_far, n_all, mid, hn, pre, hid, part, relay, parts, ended,
    lsem, send, krecv, kdrecv, wrecv, drecv, orecv, nrecv, xrecv, precv,
):
    at = Where()
    x, sp, core, other = at.x, at.sp, at.core, at.other
    rows = q.shape[1]
    own = rows // 4
    late = at.late == 1
    early = at.late == 0
    mine = at.half_chip(0, 0)

    barrier = pltpu.get_barrier_semaphore()
    after, before = lax.rem(sp + 1, 32), lax.rem(sp + 31, 32)
    for to in (other, at.step("y", True), at.step("y", False), at.step("z", True), at.step("z", False)):
        pl.semaphore_signal(barrier, inc=1, device_id={"sp": to}, device_id_type=MESH)
    for to in (after, before):
        for x_to in range(4):
            pl.semaphore_signal(barrier, inc=1, device_id={"sp": to, "tp": x_to}, device_id_type=MESH)
    xs = [lax.rem(x + d, 4) for d in range(4)]
    for to in xs[1:]:
        pl.semaphore_signal(barrier, inc=1, device_id={"tp": to}, device_id_type=MESH)

    loads = [
        pltpu.make_async_copy(src, dst, lsem.at[i])
        for i, (src, dst) in enumerate(
            (
                (k_in, k_raw), (v_in, v_raw), (q_in, q_raw), (wo_in, wo.at[x]), (wg_in, wg.at[sp]), (wu_in, wu.at[sp]),
                (wd_in, wd), (res_in, res.at[pl.ds(16, rows)]), (lam_in, lam), (sub_in, sub_gain),
                (norm_in, norm_gain), (conv_g_in, conv_g), (conv_u_in, conv_u),
            )
        )
    ]
    for load in loads[:3]:
        load.start()
    loads[0].wait()
    kbuf[mine * 2 + core] = k_raw[...].reshape(kbuf.shape[1:])
    for load in loads[3:6] + loads[7:]:
        load.start()
    with jax.named_scope("barrier"):
        pl.semaphore_wait(barrier, 16)

    keys = HalfGather(at, kbuf, send.at[0], krecv.at[0], kdrecv)
    vals = HalfGather(at, vbuf, send.at[1], krecv.at[1], kdrecv)
    gate = Gather(at, wg, "y", send.at[2], wrecv.at[0], drecv.at[0])
    up = Gather(at, wu, "z", send.at[3], wrecv.at[1], drecv.at[1])

    def key_on(dy):
        keys.out(3 + FIRST.index(dy), dy, 0, None, at.pair())

    def q_copy():
        return remote(q.at[0], q.at[1], send.at[9], orecv.at[0], sp=at.opposite())

    keys.ring_start(0, 0)
    loads[1].wait()
    vbuf[mine * 2 + core] = v_raw[...].reshape(vbuf.shape[1:])
    vals.out(0, 0, 0, None, at.pair())
    key_on(0)
    vals.ring_start(1, 0)
    keys.across(0, 0)
    vals.across(0, 0)
    loads[2].wait()
    q[0] = q_raw[...].reshape(q.shape[1:])

    @pl.when(late)
    def _():
        q_copy().start()

    def weights_along_z(forward):
        gate.start_along("g", forward)
        up.start_along("f", forward)

    loads[4].wait()
    loads[5].wait()
    for forward in (True, False):
        pl.when(at.zl == int(forward))(functools.partial(weights_along_z, forward))

    def weights_start():
        for forward in (True, False):
            up.start_along("g", forward)
            pl.when(at.zl == int(not forward))(functools.partial(weights_along_z, forward))
        gate.across(0, 0)
        up.across(0, 0)

    wo_half = wo.shape[1] // 2
    wo_quarter = wo_half // 2

    def wo_copy(ident, slot, start, size, to):
        ref = wo.at[slot, pl.ds(core * wo_half + start, size)]
        return remote(ref, ref, send.at[4], xrecv.at[ident], tp=to)

    def wo_over(slot):
        ref = wo.at[slot, pl.ds(core * wo_half, wo_half)]
        return remote(ref, ref, send.at[4], xrecv.at[3], sp=other)

    def res_copy(to):
        return remote(res.at[pl.ds(rows, 16)], res.at[pl.ds(0, 16)], send.at[6], xrecv.at[8], sp=to)

    def n_halo_copy(slot, to, x_to):
        return remote(
            n_all.at[slot, pl.ds(rows, 16)], n_all.at[slot, pl.ds(0, 16)], send.at[7], xrecv.at[9], sp=to, tp=x_to
        )

    loads[7].wait()
    loads[6].start()

    @pl.when(sp < 31)
    def _():
        res_copy(after).start()

    @pl.when(sp == 0)
    def _():
        res[:16, :] = jnp.zeros((16, res.shape[1]), BF16)
        n_all[:, :16, :] = jnp.zeros((4, 16, n_all.shape[2]), BF16)

    loads[3].wait()
    wo_copy(0, x, 0, wo_half, xs[1]).start()
    wo_copy(1, x, 0, wo_half, xs[3]).start()

    def wo_middle():
        wo_copy(0, xs[3], 0, wo_half, xs[1]).wait_recv()
        wo_copy(2, xs[3], 0, wo_quarter, xs[1]).start()
        wo_over(xs[3]).start()
        wo_copy(1, xs[1], 0, wo_half, xs[3]).wait_recv()
        wo_copy(2, xs[1], wo_quarter, wo_quarter, xs[3]).start()
        wo_over(xs[1]).start()

    def wo_end():
        wo_copy(2, xs[2], 0, wo_half, xs[1]).wait_recv()
        wo_over(xs[2]).start()

    def wo_wait():
        ref = wo.at[pl.ds(0, 3), pl.ds(0, wo_half)]
        remote(ref, ref, send.at[4], xrecv.at[3], sp=other).wait_recv()

    scale = 1.0 / math.sqrt(128.0) / math.log(2.0)

    def block(who, chip, masked):
        for j in range(4):
            h = j // 2
            kj = kbuf[pl.ds(chip * 2, 2), :, 128 * j : 128 * j + 128].reshape(2 * rows, 128)
            vj = vbuf[pl.ds(chip * 2, 2), :, 256 * h : 256 * h + 256].reshape(2 * rows, 256)
            s = lax.dot_general(
                q[who, :, 128 * j : 128 * j + 128], kj, (((1,), (1,)), ((), ())), preferred_element_type=F32
            )
            s = s * scale
            if masked:
                q_pos = lax.broadcasted_iota(jnp.int32, s.shape, 0) + core * rows
                s = jnp.where(lax.broadcasted_iota(jnp.int32, s.shape, 1) <= q_pos, s, -1e30)
            top = jnp.max(s, axis=1, keepdims=True)
            if masked:
                m_new = top
            else:
                m_old = m_s[4 * who + j][:, :1]
                m_new = jnp.maximum(m_old, top)
                alpha = jnp.exp2(m_old - m_new)
            p = jnp.exp2(s - m_new)
            part_sum = p[:, :128]
            for i in range(1, 2 * rows // 128):
                part_sum = part_sum + p[:, 128 * i : 128 * i + 128]
            pv = jnp.dot(p.astype(BF16), vj, preferred_element_type=F32)
            m_s[4 * who + j] = jnp.broadcast_to(m_new, (rows, 128))
            if masked:
                l_s[4 * who + j] = part_sum
                acc[4 * who + j] = pv
            else:
                l_s[4 * who + j] = l_s[4 * who + j] * alpha + part_sum
                acc[4 * who + j] = acc[4 * who + j] * alpha + pv

    @pl.when(early)
    def _():
        m_s[4:] = jnp.full((4, rows, 128), -1e30, F32)
        l_s[4:] = jnp.zeros((4, rows, 128), F32)
        acc[4:] = jnp.zeros((4, *acc.shape[1:]), F32)

    with jax.named_scope("own_wait"):
        keys.both_from_other(0)
    with jax.named_scope("own_block"):
        block(0, mine, True)

    def handler_0():
        keys.ring_middle(0, 0, key_on)
        vals.into(0, 0, 1)
        vals.ring_start(4, 1)
        for forward in (True, False):
            gate.start_along("f", forward)
        vals.across(0, 1)
        vals.ring_middle(1, 0)
        keys.into(3, 0, 1)
        keys.across(0, 1)

        @pl.when(early)
        def _():
            q_copy().wait_recv()

    def handler_2():
        keys.ring_end(0, 0, key_on)

    def gate_along_z(forward):
        gate.second_step(1, forward)
        gate.second_step(2, forward)

    def handler_4():
        vals.ring_middle(4, 1)
        for ident, dy in ((4, 1), (5, 3)):
            keys.into(ident, dy, 1)
            keys.across(dy, 1)

    def up_on(forward):
        up.into(0 if forward else 1, 1 if forward else 3, 0)
        up.first_step(forward)
        up.along_second(1 if forward else 2)

    def handler_5():
        gate.got_first()
        for forward in (True, False):
            pl.when(at.zl == int(forward))(functools.partial(gate_along_z, forward))
        weights_start()
        vals.ring_end(1, 0)
        for forward in (True, False):
            gate.first_step(forward)
        for forward in (True, False):
            pl.when(at.zl == int(not forward))(functools.partial(up_on, forward))
            pl.when(at.zl == int(not forward))(functools.partial(gate_along_z, forward))
        gate.across(FIRST[1], 0)
        gate.across(FIRST[2], 0)
        wo_middle()

    def handler_6():
        vals.ring_end(4, 1)
        keys.into(6, 2, 1)
        keys.across(2, 1)

    def step(t, carry):
        for when, handler in (
            (0, handler_0), (2, handler_2), (4, handler_4), (5, handler_5), (6, handler_6)
        ):

            @pl.when(t == when)
            def _():
                with jax.named_scope(handler.__name__):
                    handler()

        dy, zo = (pick(t, [d[i] for d in HALF_ORDER]) for i in (0, 1))
        chip = at.half_chip(dy, zo)

        @pl.when(t > 0)
        def _():
            with jax.named_scope("d2d_wait"):
                keys.both_from_other(t)

        @pl.when(early)
        def _():
            with jax.named_scope("far_block"):
                block(1, chip, False)

        @pl.when((chip < mine) & (late | (t < 4)))
        def _():
            with jax.named_scope("block"):
                block(0, chip, False)

        return carry

    def own_step(t, carry):
        dy, zo = (pick(t, [d[i] for d in HALF_ORDER]) for i in (0, 1))
        chip = at.half_chip(dy, zo)

        @pl.when(chip < mine)
        def _():
            with jax.named_scope("block"):
                block(0, chip, False)

        return carry

    lax.fori_loop(0, 8, step, 0)

    def stat_copy():
        return remote(stat, stat_far, send.at[10], orecv.at[1], sp=at.opposite())

    def a_copy(h):
        return remote(a_far.at[h], a_far.at[h], send.at[11], orecv.at[2 + h], sp=at.opposite())

    loads[8].wait()
    loads[9].wait()
    lanes = lax.broadcasted_iota(jnp.int32, (rows, 128), 1)
    base = 4 - 4 * at.late
    stats = jnp.zeros((rows, 128), F32)
    for j in range(4):
        total = jnp.sum(l_s[base + j], axis=1, keepdims=True)
        stats = jnp.where(lanes == j, m_s[base + j], jnp.where(lanes == 4 + j, total, stats))
    stat[...] = stats.T[:8]
    stat_copy().start()

    with jax.named_scope("w_first"):
        for forward in (True, False):
            pl.when(at.zl == int(forward))(functools.partial(up_on, forward))

    with jax.named_scope("stat_wait"):
        stat_copy().wait_recv()

    with jax.named_scope("blend"):
        here = jnp.concatenate([stat[...], jnp.zeros((120, rows), F32)], axis=0).T
        there = jnp.concatenate([stat_far[...], jnp.zeros((120, rows), F32)], axis=0).T
        for h in range(2):
            shares = []
            for j in (2 * h, 2 * h + 1):
                m_here, m_there = here[:, j : j + 1], there[:, j : j + 1]
                top = jnp.maximum(m_here, m_there)
                e_here, e_there = jnp.exp2(m_here - top), jnp.exp2(m_there - top)
                total = here[:, 4 + j : 5 + j] * e_here + there[:, 4 + j : 5 + j] * e_there
                shares.append(acc[base + j] * (e_here / total))
            a = shares[0] - lam[h] * shares[1]

            @pl.when(early)
            def _():
                a_far[h] = a.astype(BF16)
                a_copy(h).start()

            @pl.when(late)
            def _():
                acc[2 * h] = a

    @pl.when(early)
    def _():
        lax.fori_loop(4, 8, own_step, 0)

    with jax.named_scope("w_second"):
        gate.got_second(0)
        up.got_second(0)
        gate.got_opposite()
        up.got_opposite()

    def n_copy(ident, h, slot, start, size, to):
        ref = n_all.at[slot, pl.ds(16 + start, size), pl.ds(256 * h, 256)]
        return remote(ref, ref, send.at[5], nrecv.at[h, ident], tp=to)

    for h in range(2):

        @pl.when(late)
        def _():
            with jax.named_scope("a_wait"):
                a_copy(h).wait_recv()
            acc[2 * h] = acc[2 * h] + a_far[h].astype(F32)

        @pl.when(early)
        def _():
            mixed = []
            for j in (2 * h, 2 * h + 1):
                mixed.append(acc[j] / jnp.sum(l_s[j], axis=1, keepdims=True))
            acc[2 * h] = mixed[0] - lam[h] * mixed[1]

        a = acc[2 * h]
        square = jnp.mean(a * a, axis=1, keepdims=True)
        n = a * lax.rsqrt(square + EPS) * sub_gain[...] * (1.0 - LAMBDA_INIT)
        n_all[x, 16:, 256 * h : 256 * h + 256] = n.astype(BF16)
        n_copy(0, h, x, 0, rows, xs[1]).start()
        n_copy(1, h, x, 0, rows, xs[3]).start()

    @pl.when(sp < 31)
    def _():
        for x_to in range(4):
            n_halo_copy(x, after, x_to).start()

    with jax.named_scope("wo_end"):
        wo_end()
    with jax.named_scope("w_third"):
        for j in (1, 2):
            gate.got_second(j, uneven=True)
            up.got_second(j)
    with jax.named_scope("n_middle"):
        for h in range(2):
            n_copy(0, h, xs[3], 0, rows, xs[1]).wait_recv()
            n_copy(2, h, xs[3], 0, rows // 2, xs[1]).start()
            n_copy(1, h, xs[1], 0, rows, xs[3]).wait_recv()
            n_copy(2, h, xs[1], rows // 2, rows // 2, xs[3]).start()

    with jax.named_scope("w_fourth"):
        up.got_second(3)
        gate.got_second(3)

    @pl.when(sp > 0)
    def _():
        with jax.named_scope("halo_wait"):
            res_copy(before).wait_recv()
            ref = n_all.at[pl.ds(0, 4), pl.ds(0, 16)]
            remote(ref, ref, send.at[7], xrecv.at[9], sp=before).wait_recv()

    def project(slots, first):
        def body(i, carry):
            cols = pl.ds(pl.multiple_of(i * 256, 256), 256)
            sums = res[:, cols].astype(F32) if first else mid[:, cols]
            for slot in slots:
                sums = sums + jnp.dot(n_all[slot], wo[slot, :, cols], preferred_element_type=F32)
            mid[:, cols] = sums
            return carry

        lax.fori_loop(0, mid.shape[1] // 256, body, 0, unroll=2)

    with jax.named_scope("wo_wait"):
        wo_wait()
    with jax.named_scope("project"):
        project((x, xs[1], xs[3]), True)
    with jax.named_scope("n_wait"):
        for h in range(2):
            n_copy(2, h, xs[2], 0, rows, xs[1]).wait_recv()
    with jax.named_scope("project_last"):
        project((xs[2],), False)
    for load in loads[10:]:
        load.wait()
    with jax.named_scope("norm"):
        middle = mid[...]
        square = jnp.mean(middle * middle, axis=1, keepdims=True)
        hn[...] = (middle * lax.rsqrt(square + EPS) * norm_gain[...]).astype(BF16)
    feats = hn.shape[1]
    units = wg.shape[2]
    row, place = feats // 4, feats // 16

    def gate_part(dz, cols):
        z = lax.rem(at.z + dz, 4)
        return jnp.dot(
            hn[:, pl.ds(pl.multiple_of(z * row, row), row)], wg[pl.ds(z * 8, 8), :, cols].reshape(row, -1),
            preferred_element_type=F32,
        )

    def up_part(dy, cols):
        y = lax.rem(at.y + dy, 4)
        left = [hn[:, pl.ds(pl.multiple_of(z * row + y * place, place), place)] for z in range(4)]
        right = [wu[pl.ds(z * 8 + y * 2, 2), :, cols].reshape(place, -1) for z in range(4)]
        return jnp.dot(
            jnp.concatenate(left, axis=1), jnp.concatenate(right, axis=0), preferred_element_type=F32
        )

    def mix(g, taps):
        return taps[0:1] * pltpu.roll(g, 2, 0) + taps[1:2] * pltpu.roll(g, 1, 0) + taps[2:3] * g

    def feed_most(at_col, width):
        cols = pl.ds(at_col, width)
        for i, part_of in enumerate((gate_part, up_part)):
            pre[i, :, cols] = part_of(0, cols) + part_of(1, cols) + part_of(3, cols)

    def feed_last(at_col, width):
        cols = pl.ds(at_col, width)
        mixed = []
        for i, (part_of, taps) in enumerate(((gate_part, conv_g), (up_part, conv_u))):
            g = (pre[i, :, cols] + part_of(2, cols)).astype(BF16).astype(F32)
            mixed.append(mix(g, taps[:, cols])[16:])
        gc, uc = mixed
        hid[:, cols] = (gc * (0.5 + 0.5 * jnp.tanh(0.5 * gc)) * uc).astype(BF16)

    def feed(body):
        for start in range(0, units, 256):
            body(start, min(256, units - start))

    with jax.named_scope("w_rest"):
        gate.from_other(0)
        up.from_other(0)
    with jax.named_scope("feed_most"):
        feed(feed_most)
    with jax.named_scope("w_fifth"):
        for j in range(4):
            gate.got_far(j)
            up.got_far(j)
    with jax.named_scope("w_over"):
        gate.from_other(1)
        up.from_other(1)
        loads[6].wait()
    with jax.named_scope("feed"):
        feed(feed_last)

    chunks = part.shape[2] // 512
    side = own // 2

    def cols_of(i):
        return pl.ds(pl.multiple_of(i * 512, 512), 512)

    def relay_copy(s, i, to):
        return remote(
            part.at[xs[2], pl.ds(s * side, side), cols_of(i)], relay.at[s, :, cols_of(i)],
            send.at[8], precv.at[0, i], tp=to,
        )

    def part_copy(s, i, to):
        return remote(
            part.at[to, :, cols_of(i)], parts.at[s, :, cols_of(i)], send.at[8], precv.at[1, i], tp=to
        )

    def arrived(buf, which, i):
        ref = buf.at[:, :, cols_of(i)]
        remote(ref, ref, send.at[8], precv.at[which, i], tp=xs[1]).wait_recv()

    def lower(i, carry):
        cols = cols_of(i)
        full = jnp.dot(hid[...], wd[:, cols], preferred_element_type=F32).astype(BF16)
        part[:, :, cols] = full.reshape(4, own, 512)
        relay_copy(0, i, xs[1]).start()
        relay_copy(1, i, xs[3]).start()
        return carry

    with jax.named_scope("lower"):
        lax.fori_loop(0, chunks, lower, 0, unroll=True)

    def pass_on(i, carry):
        cols = cols_of(i)
        arrived(relay, 0, i)
        for s, to in ((0, xs[1]), (1, xs[3])):
            half = pl.ds(s * side, side)
            both = part[to, half, cols].astype(F32) + relay[s, :, cols].astype(F32)
            part[to, half, cols] = both.astype(BF16)
            part_copy(s, i, to).start()
        return carry

    def sent(ref, which):
        remote(ref, ref, send.at[which], xrecv.at[0], sp=other).wait_send()

    with jax.named_scope("drain"):
        for gather in (keys, vals, gate, up):
            gather.drain()
        sent(wo.at[pl.ds(0, 3)], 4)
        sent(n_all.at[pl.ds(0, 3), pl.ds(0, rows)], 5)
        stat_copy().wait_send()

        @pl.when(sp < 31)
        def _():
            sent(hn.at[pl.ds(0, 16)], 6)
            sent(n_all.at[pl.ds(0, 4), pl.ds(0, 16)], 7)

        @pl.when(late)
        def _():
            q_copy().wait_send()

        @pl.when(early)
        def _():
            sent(a_far, 11)

    with jax.named_scope("pass_on"):
        lax.fori_loop(0, chunks, pass_on, 0)

    def finish(i, carry):
        cols = cols_of(i)
        arrived(parts, 1, i)
        sums = parts[0, :, cols].astype(F32) + parts[1, :, cols].astype(F32) + part[x, :, cols].astype(F32)
        middle = mid[pl.ds(pl.multiple_of(16 + x * own, 16), own), cols]
        ended[:, cols] = (middle + sums).astype(BF16)
        pltpu.make_async_copy(ended.at[:, cols], out.at[:, cols], lsem.at[i]).start()
        return carry

    with jax.named_scope("finish"):
        lax.fori_loop(0, chunks, finish, 0)

    sent(hn.at[pl.ds(0, 3 * own)], 8)
    for i in range(chunks):
        pltpu.make_async_copy(ended.at[:, cols_of(i)], out.at[:, cols_of(i)], lsem.at[i]).wait()


def local(
    residual, queries, key_rows, values, lambda_head, sub_gain, w_out, norm_gain, w_gate, w_up, conv_gate, conv_up,
    w_down,
):
    rows = queries.shape[0]
    d = residual.shape[1]
    own = rows // 4
    heads_wide = queries.shape[1] * values.shape[2]
    units = w_gate.shape[1]
    maps = queries.shape[1] * 2
    places = 32
    hbm = pl.BlockSpec(memory_space=pl.ANY)
    dma = pltpu.SemaphoreType.DMA
    call = pl.pallas_call(
        kernel,
        out_shape=jax.ShapeDtypeStruct((own, d), BF16),
        in_specs=[hbm] * 13,
        out_specs=hbm,
        scratch_shapes=[
            pltpu.SMEM(lambda_head.shape, F32),
            pltpu.VMEM((1, *sub_gain.shape), F32),
            pltpu.VMEM((1, d), F32),
            pltpu.VMEM(conv_gate.shape, F32),
            pltpu.VMEM(conv_up.shape, F32),
            pltpu.VMEM(queries.shape, BF16),
            pltpu.VMEM(key_rows.shape, BF16),
            pltpu.VMEM(values.shape, BF16),
            pltpu.VMEM((2, rows, 512), BF16),
            pltpu.VMEM((places // 2, rows, 512), BF16),
            pltpu.VMEM((places // 2, rows, 512), BF16),
            pltpu.VMEM((places, w_gate.shape[0], units), BF16),
            pltpu.VMEM((places, w_gate.shape[0], units), BF16),
            pltpu.VMEM((4, *w_out.shape), BF16),
            pltpu.VMEM(w_down.shape, BF16),
            pltpu.VMEM((rows + 16, d), BF16),
            pltpu.VMEM((2 * maps, rows, 128), F32),
            pltpu.VMEM((2 * maps, rows, 128), F32),
            pltpu.VMEM((2 * maps, rows, values.shape[2]), F32),
            pltpu.VMEM((2, rows, values.shape[2]), BF16),
            pltpu.VMEM((8, rows), F32),
            pltpu.VMEM((8, rows), F32),
            pltpu.VMEM((4, rows + 16, heads_wide), BF16),
            pltpu.VMEM((rows + 16, d), F32),
            pltpu.VMEM((rows + 16, d), BF16),
            pltpu.VMEM((2, rows + 16, units), F32),
            pltpu.VMEM((rows, units), BF16),
            pltpu.VMEM((4, own, d), BF16),
            pltpu.VMEM((2, own // 2, d), BF16),
            pltpu.VMEM((2, own, d), BF16),
            pltpu.VMEM((own, d), BF16),
            dma((13,)), dma((12,)), dma((2, 7)), dma((8,)), dma((2, 15)), dma((2, 2)), dma((4,)), dma((2, 3)), dma((10,)),
            dma((2, d // 512)),
        ],
        compiler_params=pltpu.CompilerParams(
            collective_id=0, has_side_effects=True, vmem_limit_bytes=67043328
        ),
    )
    return call(
        lambda_head, sub_gain[None], norm_gain[None], conv_gate, conv_up,
        queries, key_rows, values,
        w_gate, w_up, w_out, w_down, residual,
    )


def solution(mesh):
    placed = (
        P("sp", None),
        P("sp", "tp", None, None),
        P("sp", "tp", None, None),
        P("sp", "tp", None),
        P("tp"),
        P(),
        P("tp", None),
        P(),
        P("sp", "tp"),
        P("sp", "tp"),
        P(None, "tp"),
        P(None, "tp"),
        P("tp", None),
    )
    return jax.shard_map(
        local, mesh=mesh, in_specs=placed, out_specs=P(("sp", "tp"), None), check_vma=False
    )
```

```python
import functools
import math

import jax
import jax.numpy as jnp
from jax import lax
from jax.experimental import pallas as pl
from jax.experimental.pallas import tpu as pltpu
from jax.sharding import PartitionSpec as P

EPS = 1e-06
LAMBDA_INIT = 0.8 - 0.6 * math.exp(-0.3)
BF16, F32 = jnp.bfloat16, jnp.float32
MESH = pl.DeviceIdType.MESH

ORDER = (
    (0, 0),
    (1, 0), (3, 0), (0, 1), (0, 3),
    (1, 1), (1, 3), (3, 1), (3, 3),
    (2, 0), (0, 2),
    (2, 1), (2, 3), (1, 2), (3, 2),
    (2, 2),
)
STEP_OF = {d: t for t, d in enumerate(ORDER)}
FIRST = (0, 1, 3, 2)
HALF_ORDER = ((0, 0), (1, 0), (3, 0), (0, 1), (1, 1), (3, 1), (2, 0), (2, 1))
HALF_STEP_OF = {d: t for t, d in enumerate(HALF_ORDER)}


def pick(t, values):
    return sum(jnp.where(t == i, v, 0) for i, v in enumerate(values) if v)


def remote(src, dst, send, recv, **to):
    return pltpu.make_async_remote_copy(
        src_ref=src, dst_ref=dst, send_sem=send, recv_sem=recv, device_id=to, device_id_type=MESH
    )


class Where:
    def __init__(self):
        self.sp = lax.axis_index("sp")
        self.x = lax.axis_index("tp")
        self.core = lax.rem(self.sp, 2)
        self.other = self.sp + 1 - 2 * self.core
        self.chip = self.sp // 2
        self.y = lax.rem(self.chip, 4)
        self.z = self.chip // 4
        self.zl = lax.rem(self.z, 2)
        self.late = self.z // 2

    def chip_behind(self, dy, dz):
        return lax.rem(self.z + 4 - dz, 4) * 4 + lax.rem(self.y + 4 - dy, 4)

    def step(self, axis, forward):
        d = 3 if forward else 1
        return (self.chip_behind(d, 0) if axis == "y" else self.chip_behind(0, d)) * 2 + self.core

    def pair(self):
        return ((self.z + 1 - 2 * self.zl) * 4 + self.y) * 2 + self.core

    def opposite(self):
        return ((3 - self.z) * 4 + self.y) * 2 + self.core

    def half_chip(self, dy, zo):
        zl = self.zl + zo - 2 * zo * self.zl
        return zl * 4 + lax.rem(self.y + 4 - dy, 4)


class Gather:
    def __init__(self, at, buf, first, send, recv, drecv):
        self.at, self.buf, self.send, self.recv, self.drecv = at, buf, send, recv, drecv
        self.axes = {"f": first, "g": "z" if first == "y" else "y"}
        self.half = buf.shape[1] // 2

    def slot(self, df, dg):
        dy, dz = (df, dg) if self.axes["f"] == "y" else (dg, df)
        return self.at.chip_behind(dy, dz) * 2 + self.at.core

    def copy(self, ident, slot, half, to):
        ref = self.buf.at[slot]
        if half is not None:
            ref = self.buf.at[slot, pl.ds(half * self.half, self.half)]
        return remote(ref, ref, self.send, self.recv.at[ident], sp=to)

    def out(self, ident, df, dg, half, axis, forward):
        self.copy(ident, self.slot(df, dg), half, self.at.step(self.axes[axis], forward)).start()

    def into(self, ident, df, dg):
        self.copy(ident, self.slot(df, dg), None, self.at.other).wait_recv()

    def across(self, df, dg, far=0):
        ref = self.buf.at[self.slot(df, dg)]
        remote(ref, ref, self.send, self.drecv.at[far], sp=self.at.other).start()

    def start_along(self, axis, forward):
        self.out((0 if axis == "f" else 3) + (not forward), 0, 0, None, axis, forward)

    def along_second(self, j):
        self.second_step(j, True)
        self.second_step(j, False)
        self.across(FIRST[j], 0)

    def second_step(self, j, forward):
        self.out((3 if forward else 4) + 3 * j, FIRST[j], 0, None, "g", forward)

    def got_first(self):
        self.into(0, 1, 0)
        self.into(1, 3, 0)

    def first_step(self, forward):
        if forward:
            self.out(2, 1, 0, 0, "f", True)
        else:
            self.out(2, 3, 0, 1, "f", False)

    def got_second(self, j, uneven=False):
        self.into(3 + 3 * j, FIRST[j], 1)
        self.into(4 + 3 * j, FIRST[j], 3)

        def pass_on(cut):
            for df, dg, start, stop in ((FIRST[j], 1, 0, cut), (FIRST[j], 3, cut, 2 * self.half)):
                ref = self.buf.at[self.slot(df, dg), pl.ds(start, stop - start)]
                to = self.at.step(self.axes["g"], dg == 1)
                remote(ref, ref, self.send, self.recv.at[5 + 3 * j], sp=to).start()

        if uneven:
            for zl, cut in ((0, self.half // 2), (1, 3 * self.half // 2)):
                pl.when(self.at.zl == zl)(functools.partial(pass_on, cut))
        else:
            pass_on(self.half)
        self.across(FIRST[j], 1)
        self.across(FIRST[j], 3)

    def got_opposite(self):
        self.into(2, 2, 0)
        self.along_second(3)

    def got_far(self, j):
        self.into(5 + 3 * j, FIRST[j], 2)
        self.across(FIRST[j], 2, 1)

    def from_other(self, far):
        ref = self.buf.at[pl.ds(0, 4 if far else 12)]
        remote(ref, ref, self.send, self.drecv.at[far], sp=self.at.other).wait_recv()

    def drain(self):
        ref = self.buf.at[pl.ds(0, 31)]
        remote(ref, ref, self.send, self.drecv.at[0], sp=self.at.other).wait_send()


class HalfGather:
    def __init__(self, at, buf, send, recv, drecv):
        self.at, self.buf, self.send, self.recv, self.drecv = at, buf, send, recv, drecv
        self.half = buf.shape[1] // 2

    def slot(self, dy, zo):
        return self.at.half_chip(dy, zo) * 2 + self.at.core

    def copy(self, ident, dy, zo, half, to):
        ref = self.buf.at[self.slot(dy, zo)]
        if half is not None:
            ref = self.buf.at[self.slot(dy, zo), pl.ds(half * self.half, self.half)]
        return remote(ref, ref, self.send, self.recv.at[ident], sp=to)

    def out(self, ident, dy, zo, half, to):
        self.copy(ident, dy, zo, half, to).start()

    def into(self, ident, dy, zo):
        self.copy(ident, dy, zo, None, self.at.other).wait_recv()

    def over(self, t, slot):
        ref = self.buf.at[slot]
        return remote(ref, ref, self.send, self.drecv.at[t], sp=self.at.other)

    def across(self, dy, zo):
        self.over(HALF_STEP_OF[dy, zo], self.slot(dy, zo)).start()

    def both_from_other(self, t):
        ref = self.buf.at[pl.ds(0, 2)]
        remote(ref, ref, self.send, self.drecv.at[t], sp=self.at.other).wait_recv()

    def ring_start(self, ident, zo):
        self.out(ident, 0, zo, None, self.at.step("y", True))
        self.out(ident + 1, 0, zo, None, self.at.step("y", False))

    def ring_middle(self, ident, zo, after=lambda dy: None):
        self.into(ident, 1, zo)
        self.out(ident + 2, 1, zo, 0, self.at.step("y", True))
        after(1)
        self.across(1, zo)
        self.into(ident + 1, 3, zo)
        self.out(ident + 2, 3, zo, 1, self.at.step("y", False))
        after(3)
        self.across(3, zo)

    def ring_end(self, ident, zo, after=lambda dy: None):
        self.into(ident + 2, 2, zo)
        after(2)
        self.across(2, zo)

    def drain(self):
        ref = self.buf.at[pl.ds(0, 15)]
        remote(ref, ref, self.send, self.recv.at[0], sp=self.at.other).wait_send()


def kernel(
    lam_in, sub_in, norm_in, conv_g_in, conv_u_in,
    q_in, k_in, v_in, wg_in, wu_in, wo_in, wd_in, res_in,
    out,
    lam, sub_gain, norm_gain, conv_g, conv_u, q_raw, k_raw, v_raw, q, kbuf, vbuf, wg, wu, wo, wd, res,
    m_s, l_s, acc, a_far, stat, stat_far, n_all, mid, hn, pre, hid, part, relay, parts, ended,
    lsem, send, krecv, kdrecv, wrecv, drecv, orecv, nrecv, xrecv, precv,
):
    at = Where()
    x, sp, core, other = at.x, at.sp, at.core, at.other
    rows = q.shape[1]
    own = rows // 4
    late = at.late == 1
    early = at.late == 0
    mine = at.half_chip(0, 0)

    barrier = pltpu.get_barrier_semaphore()
    after, before = lax.rem(sp + 1, 32), lax.rem(sp + 31, 32)
    for to in (other, at.step("y", True), at.step("y", False), at.step("z", True), at.step("z", False)):
        pl.semaphore_signal(barrier, inc=1, device_id={"sp": to}, device_id_type=MESH)
    for to in (after, before):
        for x_to in range(4):
            pl.semaphore_signal(barrier, inc=1, device_id={"sp": to, "tp": x_to}, device_id_type=MESH)
    xs = [lax.rem(x + d, 4) for d in range(4)]
    for to in xs[1:]:
        pl.semaphore_signal(barrier, inc=1, device_id={"tp": to}, device_id_type=MESH)

    loads = [
        pltpu.make_async_copy(src, dst, lsem.at[i])
        for i, (src, dst) in enumerate(
            (
                (k_in, k_raw), (v_in, v_raw), (q_in, q_raw), (wo_in, wo.at[x]), (wg_in, wg.at[sp]), (wu_in, wu.at[sp]),
                (wd_in, wd), (res_in, res.at[pl.ds(16, rows)]), (lam_in, lam), (sub_in, sub_gain),
                (norm_in, norm_gain), (conv_g_in, conv_g), (conv_u_in, conv_u),
            )
        )
    ]
    for load in loads[:3]:
        load.start()
    loads[0].wait()
    kbuf[mine * 2 + core] = k_raw[...].reshape(kbuf.shape[1:])
    for load in loads[3:6] + loads[7:]:
        load.start()
    with jax.named_scope("barrier"):
        pl.semaphore_wait(barrier, 16)

    keys = HalfGather(at, kbuf, send.at[0], krecv.at[0], kdrecv)
    vals = HalfGather(at, vbuf, send.at[1], krecv.at[1], kdrecv)
    gate = Gather(at, wg, "y", send.at[2], wrecv.at[0], drecv.at[0])
    up = Gather(at, wu, "z", send.at[3], wrecv.at[1], drecv.at[1])

    def key_on(dy):
        keys.out(3 + FIRST.index(dy), dy, 0, None, at.pair())

    def q_copy():
        return remote(q.at[0], q.at[1], send.at[9], orecv.at[0], sp=at.opposite())

    keys.ring_start(0, 0)
    loads[1].wait()
    vbuf[mine * 2 + core] = v_raw[...].reshape(vbuf.shape[1:])
    vals.out(0, 0, 0, None, at.pair())
    key_on(0)
    vals.ring_start(1, 0)
    keys.across(0, 0)
    vals.across(0, 0)
    loads[2].wait()
    q[0] = q_raw[...].reshape(q.shape[1:])

    @pl.when(late)
    def _():
        q_copy().start()

    def weights_along_z(forward):
        up.start_along("f", forward)
        gate.start_along("g", forward)

    loads[4].wait()
    loads[5].wait()
    for forward in (True, False):
        pl.when(at.zl == int(forward))(functools.partial(weights_along_z, forward))

    def weights_start():
        for forward in (True, False):
            up.start_along("g", forward)
            pl.when(at.zl == int(not forward))(functools.partial(weights_along_z, forward))
        gate.across(0, 0)
        up.across(0, 0)

    wo_half = wo.shape[1] // 2
    wo_quarter = wo_half // 2

    def wo_copy(ident, slot, start, size, to):
        ref = wo.at[slot, pl.ds(core * wo_half + start, size)]
        return remote(ref, ref, send.at[4], xrecv.at[ident], tp=to)

    def wo_over(slot):
        ref = wo.at[slot, pl.ds(core * wo_half, wo_half)]
        return remote(ref, ref, send.at[4], xrecv.at[3], sp=other)

    def res_copy(to):
        return remote(res.at[pl.ds(rows, 16)], res.at[pl.ds(0, 16)], send.at[6], xrecv.at[8], sp=to)

    def n_halo_copy(slot, to, x_to):
        return remote(
            n_all.at[slot, pl.ds(rows, 16)], n_all.at[slot, pl.ds(0, 16)], send.at[7], xrecv.at[9], sp=to, tp=x_to
        )

    loads[7].wait()
    loads[6].start()

    @pl.when(sp < 31)
    def _():
        res_copy(after).start()

    @pl.when(sp == 0)
    def _():
        res[:16, :] = jnp.zeros((16, res.shape[1]), BF16)
        n_all[:, :16, :] = jnp.zeros((4, 16, n_all.shape[2]), BF16)

    loads[3].wait()
    wo_copy(0, x, 0, wo_half, xs[1]).start()
    wo_copy(1, x, 0, wo_half, xs[3]).start()

    def wo_middle():
        wo_copy(0, xs[3], 0, wo_half, xs[1]).wait_recv()
        wo_copy(2, xs[3], 0, wo_quarter, xs[1]).start()
        wo_over(xs[3]).start()
        wo_copy(1, xs[1], 0, wo_half, xs[3]).wait_recv()
        wo_copy(2, xs[1], wo_quarter, wo_quarter, xs[3]).start()
        wo_over(xs[1]).start()

    def wo_end():
        wo_copy(2, xs[2], 0, wo_half, xs[1]).wait_recv()
        wo_over(xs[2]).start()

    def wo_wait():
        ref = wo.at[pl.ds(0, 3), pl.ds(0, wo_half)]
        remote(ref, ref, send.at[4], xrecv.at[3], sp=other).wait_recv()

    scale = 1.0 / math.sqrt(128.0) / math.log(2.0)

    def block(who, chip, masked):
        for j in range(4):
            h = j // 2
            kj = kbuf[pl.ds(chip * 2, 2), :, 128 * j : 128 * j + 128].reshape(2 * rows, 128)
            vj = vbuf[pl.ds(chip * 2, 2), :, 256 * h : 256 * h + 256].reshape(2 * rows, 256)
            s = lax.dot_general(
                q[who, :, 128 * j : 128 * j + 128], kj, (((1,), (1,)), ((), ())), preferred_element_type=F32
            )
            s = s * scale
            if masked:
                q_pos = lax.broadcasted_iota(jnp.int32, s.shape, 0) + core * rows
                s = jnp.where(lax.broadcasted_iota(jnp.int32, s.shape, 1) <= q_pos, s, -1e30)
            top = jnp.max(s, axis=1, keepdims=True)
            if masked:
                m_new = top
            else:
                m_old = m_s[4 * who + j][:, :1]
                m_new = jnp.maximum(m_old, top)
                alpha = jnp.exp2(m_old - m_new)
            p = jnp.exp2(s - m_new)
            part_sum = p[:, :128]
            for i in range(1, 2 * rows // 128):
                part_sum = part_sum + p[:, 128 * i : 128 * i + 128]
            pv = jnp.dot(p.astype(BF16), vj, preferred_element_type=F32)
            m_s[4 * who + j] = jnp.broadcast_to(m_new, (rows, 128))
            if masked:
                l_s[4 * who + j] = part_sum
                acc[4 * who + j] = pv
            else:
                l_s[4 * who + j] = l_s[4 * who + j] * alpha + part_sum
                acc[4 * who + j] = acc[4 * who + j] * alpha + pv

    @pl.when(early)
    def _():
        m_s[4:] = jnp.full((4, rows, 128), -1e30, F32)
        l_s[4:] = jnp.zeros((4, rows, 128), F32)
        acc[4:] = jnp.zeros((4, *acc.shape[1:]), F32)

    with jax.named_scope("own_wait"):
        keys.both_from_other(0)
    with jax.named_scope("own_block"):
        block(0, mine, True)

    def handler_0():
        keys.ring_middle(0, 0, key_on)
        vals.into(0, 0, 1)
        vals.ring_start(4, 1)
        for forward in (True, False):
            gate.start_along("f", forward)
        vals.across(0, 1)
        vals.ring_middle(1, 0)
        keys.into(3, 0, 1)
        keys.across(0, 1)

        @pl.when(early)
        def _():
            q_copy().wait_recv()

    def handler_2():
        keys.ring_end(0, 0, key_on)

    def gate_along_z(forward):
        gate.second_step(1, forward)
        gate.second_step(2, forward)

    def handler_4():
        vals.ring_middle(4, 1)
        for ident, dy in ((4, 1), (5, 3)):
            keys.into(ident, dy, 1)
            keys.across(dy, 1)

    def up_on(forward):
        up.into(0 if forward else 1, 1 if forward else 3, 0)
        up.first_step(forward)
        up.along_second(1 if forward else 2)

    def handler_5():
        gate.got_first()
        for forward in (True, False):
            pl.when(at.zl == int(forward))(functools.partial(gate_along_z, forward))
        weights_start()
        vals.ring_end(1, 0)
        for forward in (True, False):
            gate.first_step(forward)
        for forward in (True, False):
            pl.when(at.zl == int(not forward))(functools.partial(up_on, forward))
            pl.when(at.zl == int(not forward))(functools.partial(gate_along_z, forward))
        gate.across(FIRST[1], 0)
        gate.across(FIRST[2], 0)
        wo_middle()

    def handler_6():
        vals.ring_end(4, 1)
        keys.into(6, 2, 1)
        keys.across(2, 1)

    def step(t, carry):
        for when, handler in (
            (0, handler_0), (2, handler_2), (4, handler_4), (5, handler_5), (6, handler_6)
        ):

            @pl.when(t == when)
            def _():
                with jax.named_scope(handler.__name__):
                    handler()

        dy, zo = (pick(t, [d[i] for d in HALF_ORDER]) for i in (0, 1))
        chip = at.half_chip(dy, zo)

        @pl.when(t > 0)
        def _():
            with jax.named_scope("d2d_wait"):
                keys.both_from_other(t)

        @pl.when(early)
        def _():
            with jax.named_scope("far_block"):
                block(1, chip, False)

        @pl.when((chip < mine) & (late | (t < 4)))
        def _():
            with jax.named_scope("block"):
                block(0, chip, False)

        return carry

    def own_step(t, carry):
        dy, zo = (pick(t, [d[i] for d in HALF_ORDER]) for i in (0, 1))
        chip = at.half_chip(dy, zo)

        @pl.when(chip < mine)
        def _():
            with jax.named_scope("block"):
                block(0, chip, False)

        return carry

    lax.fori_loop(0, 8, step, 0)

    def stat_copy():
        return remote(stat, stat_far, send.at[10], orecv.at[1], sp=at.opposite())

    def a_copy(h):
        return remote(a_far.at[h], a_far.at[h], send.at[11], orecv.at[2 + h], sp=at.opposite())

    loads[8].wait()
    loads[9].wait()
    lanes = lax.broadcasted_iota(jnp.int32, (rows, 128), 1)
    base = 4 - 4 * at.late
    stats = jnp.zeros((rows, 128), F32)
    for j in range(4):
        total = jnp.sum(l_s[base + j], axis=1, keepdims=True)
        stats = jnp.where(lanes == j, m_s[base + j], jnp.where(lanes == 4 + j, total, stats))
    stat[...] = stats.T[:8]
    stat_copy().start()

    with jax.named_scope("w_first"):
        for forward in (True, False):
            pl.when(at.zl == int(forward))(functools.partial(up_on, forward))

    with jax.named_scope("stat_wait"):
        stat_copy().wait_recv()

    with jax.named_scope("blend"):
        here = jnp.concatenate([stat[...], jnp.zeros((120, rows), F32)], axis=0).T
        there = jnp.concatenate([stat_far[...], jnp.zeros((120, rows), F32)], axis=0).T
        for h in range(2):
            shares = []
            for j in (2 * h, 2 * h + 1):
                m_here, m_there = here[:, j : j + 1], there[:, j : j + 1]
                top = jnp.maximum(m_here, m_there)
                e_here, e_there = jnp.exp2(m_here - top), jnp.exp2(m_there - top)
                total = here[:, 4 + j : 5 + j] * e_here + there[:, 4 + j : 5 + j] * e_there
                shares.append(acc[base + j] * (e_here / total))
            a = shares[0] - lam[h] * shares[1]

            @pl.when(early)
            def _():
                a_far[h] = a.astype(BF16)
                a_copy(h).start()

            @pl.when(late)
            def _():
                acc[2 * h] = a

    @pl.when(early)
    def _():
        lax.fori_loop(4, 8, own_step, 0)

    with jax.named_scope("w_second"):
        gate.got_second(0)
        up.got_second(0)
        gate.got_opposite()
        up.got_opposite()

    def n_copy(ident, h, slot, start, size, to):
        ref = n_all.at[slot, pl.ds(16 + start, size), pl.ds(256 * h, 256)]
        return remote(ref, ref, send.at[5], nrecv.at[h, ident], tp=to)

    for h in range(2):

        @pl.when(late)
        def _():
            with jax.named_scope("a_wait"):
                a_copy(h).wait_recv()
            acc[2 * h] = acc[2 * h] + a_far[h].astype(F32)

        @pl.when(early)
        def _():
            mixed = []
            for j in (2 * h, 2 * h + 1):
                mixed.append(acc[j] / jnp.sum(l_s[j], axis=1, keepdims=True))
            acc[2 * h] = mixed[0] - lam[h] * mixed[1]

        a = acc[2 * h]
        square = jnp.mean(a * a, axis=1, keepdims=True)
        n = a * lax.rsqrt(square + EPS) * sub_gain[...] * (1.0 - LAMBDA_INIT)
        n_all[x, 16:, 256 * h : 256 * h + 256] = n.astype(BF16)
        n_copy(0, h, x, 0, rows, xs[1]).start()
        n_copy(1, h, x, 0, rows, xs[3]).start()

    @pl.when(sp < 31)
    def _():
        for x_to in range(4):
            n_halo_copy(x, after, x_to).start()

    with jax.named_scope("wo_end"):
        wo_end()
    with jax.named_scope("w_third"):
        for j in (1, 2):
            gate.got_second(j, uneven=True)
            up.got_second(j)
    with jax.named_scope("n_middle"):
        for h in range(2):
            n_copy(0, h, xs[3], 0, rows, xs[1]).wait_recv()
            n_copy(2, h, xs[3], 0, rows // 2, xs[1]).start()
            n_copy(1, h, xs[1], 0, rows, xs[3]).wait_recv()
            n_copy(2, h, xs[1], rows // 2, rows // 2, xs[3]).start()

    with jax.named_scope("w_fourth"):
        up.got_second(3)
        gate.got_second(3)

    @pl.when(sp > 0)
    def _():
        with jax.named_scope("halo_wait"):
            res_copy(before).wait_recv()
            ref = n_all.at[pl.ds(0, 4), pl.ds(0, 16)]
            remote(ref, ref, send.at[7], xrecv.at[9], sp=before).wait_recv()

    def project(slots, first):
        def body(i, carry):
            cols = pl.ds(pl.multiple_of(i * 256, 256), 256)
            sums = res[:, cols].astype(F32) if first else mid[:, cols]
            for slot in slots:
                sums = sums + jnp.dot(n_all[slot], wo[slot, :, cols], preferred_element_type=F32)
            mid[:, cols] = sums
            return carry

        lax.fori_loop(0, mid.shape[1] // 256, body, 0, unroll=2)

    with jax.named_scope("wo_wait"):
        wo_wait()
    with jax.named_scope("project"):
        project((x, xs[1], xs[3]), True)
    with jax.named_scope("n_wait"):
        for h in range(2):
            n_copy(2, h, xs[2], 0, rows, xs[1]).wait_recv()
    with jax.named_scope("project_last"):
        project((xs[2],), False)
    for load in loads[10:]:
        load.wait()
    with jax.named_scope("norm"):
        middle = mid[...]
        square = jnp.mean(middle * middle, axis=1, keepdims=True)
        hn[...] = (middle * lax.rsqrt(square + EPS) * norm_gain[...]).astype(BF16)
    feats = hn.shape[1]
    units = wg.shape[2]
    row, place = feats // 4, feats // 16

    def gate_part(dz, cols):
        z = lax.rem(at.z + dz, 4)
        return jnp.dot(
            hn[:, pl.ds(pl.multiple_of(z * row, row), row)], wg[pl.ds(z * 8, 8), :, cols].reshape(row, -1),
            preferred_element_type=F32,
        )

    def up_part(dy, cols):
        y = lax.rem(at.y + dy, 4)
        left = [hn[:, pl.ds(pl.multiple_of(z * row + y * place, place), place)] for z in range(4)]
        right = [wu[pl.ds(z * 8 + y * 2, 2), :, cols].reshape(place, -1) for z in range(4)]
        return jnp.dot(
            jnp.concatenate(left, axis=1), jnp.concatenate(right, axis=0), preferred_element_type=F32
        )

    def mix(g, taps):
        return taps[0:1] * pltpu.roll(g, 2, 0) + taps[1:2] * pltpu.roll(g, 1, 0) + taps[2:3] * g

    def feed_most(at_col, width):
        cols = pl.ds(at_col, width)
        for i, part_of in enumerate((gate_part, up_part)):
            pre[i, :, cols] = part_of(0, cols) + part_of(1, cols) + part_of(3, cols)

    def feed_last(at_col, width):
        cols = pl.ds(at_col, width)
        mixed = []
        for i, (part_of, taps) in enumerate(((gate_part, conv_g), (up_part, conv_u))):
            g = (pre[i, :, cols] + part_of(2, cols)).astype(BF16).astype(F32)
            mixed.append(mix(g, taps[:, cols])[16:])
        gc, uc = mixed
        hid[:, cols] = (gc * (0.5 + 0.5 * jnp.tanh(0.5 * gc)) * uc).astype(BF16)

    def feed(body):
        for start in range(0, units, 256):
            body(start, min(256, units - start))

    with jax.named_scope("w_far"):
        for j in (0, 1):
            gate.got_far(j)
            up.got_far(j)
    with jax.named_scope("w_rest"):
        gate.from_other(0)
        up.from_other(0)
    with jax.named_scope("feed_most"):
        feed(feed_most)
    with jax.named_scope("w_fifth"):
        for j in (2, 3):
            gate.got_far(j)
            up.got_far(j)
    with jax.named_scope("w_over"):
        gate.from_other(1)
        up.from_other(1)
        loads[6].wait()
    with jax.named_scope("feed"):
        feed(feed_last)

    chunks = part.shape[2] // 512
    side = own // 2

    def cols_of(i):
        return pl.ds(pl.multiple_of(i * 512, 512), 512)

    def relay_copy(s, i, to):
        return remote(
            part.at[xs[2], pl.ds(s * side, side), cols_of(i)], relay.at[s, :, cols_of(i)],
            send.at[8], precv.at[0, i], tp=to,
        )

    def part_copy(s, i, to):
        return remote(
            part.at[to, :, cols_of(i)], parts.at[s, :, cols_of(i)], send.at[8], precv.at[1, i], tp=to
        )

    def arrived(buf, which, i):
        ref = buf.at[:, :, cols_of(i)]
        remote(ref, ref, send.at[8], precv.at[which, i], tp=xs[1]).wait_recv()

    def lower(i, carry):
        cols = cols_of(i)
        full = jnp.dot(hid[...], wd[:, cols], preferred_element_type=F32).astype(BF16)
        part[:, :, cols] = full.reshape(4, own, 512)
        relay_copy(0, i, xs[1]).start()
        relay_copy(1, i, xs[3]).start()
        return carry

    with jax.named_scope("lower"):
        lax.fori_loop(0, chunks, lower, 0, unroll=True)

    def pass_on(i, carry):
        cols = cols_of(i)
        arrived(relay, 0, i)
        for s, to in ((0, xs[1]), (1, xs[3])):
            half = pl.ds(s * side, side)
            both = part[to, half, cols].astype(F32) + relay[s, :, cols].astype(F32)
            part[to, half, cols] = both.astype(BF16)
            part_copy(s, i, to).start()
        return carry

    def sent(ref, which):
        remote(ref, ref, send.at[which], xrecv.at[0], sp=other).wait_send()

    with jax.named_scope("drain"):
        for gather in (keys, vals, gate, up):
            gather.drain()
        sent(wo.at[pl.ds(0, 3)], 4)
        sent(n_all.at[pl.ds(0, 3), pl.ds(0, rows)], 5)
        stat_copy().wait_send()

        @pl.when(sp < 31)
        def _():
            sent(hn.at[pl.ds(0, 16)], 6)
            sent(n_all.at[pl.ds(0, 4), pl.ds(0, 16)], 7)

        @pl.when(late)
        def _():
            q_copy().wait_send()

        @pl.when(early)
        def _():
            sent(a_far, 11)

    with jax.named_scope("pass_on"):
        lax.fori_loop(0, chunks, pass_on, 0)

    def finish(i, carry):
        cols = cols_of(i)
        arrived(parts, 1, i)
        sums = parts[0, :, cols].astype(F32) + parts[1, :, cols].astype(F32) + part[x, :, cols].astype(F32)
        middle = mid[pl.ds(pl.multiple_of(16 + x * own, 16), own), cols]
        ended[:, cols] = (middle + sums).astype(BF16)
        pltpu.make_async_copy(ended.at[:, cols], out.at[:, cols], lsem.at[i]).start()
        return carry

    with jax.named_scope("finish"):
        lax.fori_loop(0, chunks, finish, 0)

    sent(hn.at[pl.ds(0, 3 * own)], 8)
    for i in range(chunks):
        pltpu.make_async_copy(ended.at[:, cols_of(i)], out.at[:, cols_of(i)], lsem.at[i]).wait()


def local(
    residual, queries, key_rows, values, lambda_head, sub_gain, w_out, norm_gain, w_gate, w_up, conv_gate, conv_up,
    w_down,
):
    rows = queries.shape[0]
    d = residual.shape[1]
    own = rows // 4
    heads_wide = queries.shape[1] * values.shape[2]
    units = w_gate.shape[1]
    maps = queries.shape[1] * 2
    places = 32
    hbm = pl.BlockSpec(memory_space=pl.ANY)
    dma = pltpu.SemaphoreType.DMA
    call = pl.pallas_call(
        kernel,
        out_shape=jax.ShapeDtypeStruct((own, d), BF16),
        in_specs=[hbm] * 13,
        out_specs=hbm,
        scratch_shapes=[
            pltpu.SMEM(lambda_head.shape, F32),
            pltpu.VMEM((1, *sub_gain.shape), F32),
            pltpu.VMEM((1, d), F32),
            pltpu.VMEM(conv_gate.shape, F32),
            pltpu.VMEM(conv_up.shape, F32),
            pltpu.VMEM(queries.shape, BF16),
            pltpu.VMEM(key_rows.shape, BF16),
            pltpu.VMEM(values.shape, BF16),
            pltpu.VMEM((2, rows, 512), BF16),
            pltpu.VMEM((places // 2, rows, 512), BF16),
            pltpu.VMEM((places // 2, rows, 512), BF16),
            pltpu.VMEM((places, w_gate.shape[0], units), BF16),
            pltpu.VMEM((places, w_gate.shape[0], units), BF16),
            pltpu.VMEM((4, *w_out.shape), BF16),
            pltpu.VMEM(w_down.shape, BF16),
            pltpu.VMEM((rows + 16, d), BF16),
            pltpu.VMEM((2 * maps, rows, 128), F32),
            pltpu.VMEM((2 * maps, rows, 128), F32),
            pltpu.VMEM((2 * maps, rows, values.shape[2]), F32),
            pltpu.VMEM((2, rows, values.shape[2]), BF16),
            pltpu.VMEM((8, rows), F32),
            pltpu.VMEM((8, rows), F32),
            pltpu.VMEM((4, rows + 16, heads_wide), BF16),
            pltpu.VMEM((rows + 16, d), F32),
            pltpu.VMEM((rows + 16, d), BF16),
            pltpu.VMEM((2, rows + 16, units), F32),
            pltpu.VMEM((rows, units), BF16),
            pltpu.VMEM((4, own, d), BF16),
            pltpu.VMEM((2, own // 2, d), BF16),
            pltpu.VMEM((2, own, d), BF16),
            pltpu.VMEM((own, d), BF16),
            dma((13,)), dma((12,)), dma((2, 7)), dma((8,)), dma((2, 15)), dma((2, 2)), dma((4,)), dma((2, 3)), dma((10,)),
            dma((2, d // 512)),
        ],
        compiler_params=pltpu.CompilerParams(
            collective_id=0, has_side_effects=True, vmem_limit_bytes=67043328
        ),
    )
    return call(
        lambda_head, sub_gain[None], norm_gain[None], conv_gate, conv_up,
        queries, key_rows, values,
        w_gate, w_up, w_out, w_down, residual,
    )


def solution(mesh):
    placed = (
        P("sp", None),
        P("sp", "tp", None, None),
        P("sp", "tp", None, None),
        P("sp", "tp", None),
        P("tp"),
        P(),
        P("tp", None),
        P(),
        P("sp", "tp"),
        P("sp", "tp"),
        P(None, "tp"),
        P(None, "tp"),
        P("tp", None),
    )
    return jax.shard_map(
        local, mesh=mesh, in_specs=placed, out_specs=P(("sp", "tp"), None), check_vma=False
    )
```

```python
import functools
import math

import jax
import jax.numpy as jnp
from jax import lax
from jax.experimental import pallas as pl
from jax.experimental.pallas import tpu as pltpu
from jax.sharding import PartitionSpec as P

EPS = 1e-06
LAMBDA_INIT = 0.8 - 0.6 * math.exp(-0.3)
BF16, F32 = jnp.bfloat16, jnp.float32
MESH = pl.DeviceIdType.MESH

ORDER = (
    (0, 0),
    (1, 0), (3, 0), (0, 1), (0, 3),
    (1, 1), (1, 3), (3, 1), (3, 3),
    (2, 0), (0, 2),
    (2, 1), (2, 3), (1, 2), (3, 2),
    (2, 2),
)
STEP_OF = {d: t for t, d in enumerate(ORDER)}
FIRST = (0, 1, 3, 2)
HALF_ORDER = ((0, 0), (1, 0), (3, 0), (0, 1), (1, 1), (3, 1), (2, 0), (2, 1))
HALF_STEP_OF = {d: t for t, d in enumerate(HALF_ORDER)}


def pick(t, values):
    return sum(jnp.where(t == i, v, 0) for i, v in enumerate(values) if v)


def remote(src, dst, send, recv, **to):
    return pltpu.make_async_remote_copy(
        src_ref=src, dst_ref=dst, send_sem=send, recv_sem=recv, device_id=to, device_id_type=MESH
    )


class Where:
    def __init__(self):
        self.sp = lax.axis_index("sp")
        self.x = lax.axis_index("tp")
        self.core = lax.rem(self.sp, 2)
        self.other = self.sp + 1 - 2 * self.core
        self.chip = self.sp // 2
        self.y = lax.rem(self.chip, 4)
        self.z = self.chip // 4
        self.zl = lax.rem(self.z, 2)
        self.late = self.z // 2

    def chip_behind(self, dy, dz):
        return lax.rem(self.z + 4 - dz, 4) * 4 + lax.rem(self.y + 4 - dy, 4)

    def step(self, axis, forward):
        d = 3 if forward else 1
        return (self.chip_behind(d, 0) if axis == "y" else self.chip_behind(0, d)) * 2 + self.core

    def pair(self):
        return ((self.z + 1 - 2 * self.zl) * 4 + self.y) * 2 + self.core

    def opposite(self):
        return ((3 - self.z) * 4 + self.y) * 2 + self.core

    def half_chip(self, dy, zo):
        zl = self.zl + zo - 2 * zo * self.zl
        return zl * 4 + lax.rem(self.y + 4 - dy, 4)


class Gather:
    def __init__(self, at, buf, first, send, recv, drecv):
        self.at, self.buf, self.send, self.recv, self.drecv = at, buf, send, recv, drecv
        self.axes = {"f": first, "g": "z" if first == "y" else "y"}
        self.half = buf.shape[1] // 2

    def slot(self, df, dg):
        dy, dz = (df, dg) if self.axes["f"] == "y" else (dg, df)
        return self.at.chip_behind(dy, dz) * 2 + self.at.core

    def copy(self, ident, slot, half, to):
        ref = self.buf.at[slot]
        if half is not None:
            ref = self.buf.at[slot, pl.ds(half * self.half, self.half)]
        return remote(ref, ref, self.send, self.recv.at[ident], sp=to)

    def out(self, ident, df, dg, half, axis, forward):
        self.copy(ident, self.slot(df, dg), half, self.at.step(self.axes[axis], forward)).start()

    def into(self, ident, df, dg):
        self.copy(ident, self.slot(df, dg), None, self.at.other).wait_recv()

    def across(self, df, dg, far=0):
        ref = self.buf.at[self.slot(df, dg)]
        remote(ref, ref, self.send, self.drecv.at[far], sp=self.at.other).start()

    def start_along(self, axis, forward):
        self.out((0 if axis == "f" else 3) + (not forward), 0, 0, None, axis, forward)

    def along_second(self, j):
        self.second_step(j, True)
        self.second_step(j, False)
        self.across(FIRST[j], 0)

    def second_step(self, j, forward):
        self.out((3 if forward else 4) + 3 * j, FIRST[j], 0, None, "g", forward)

    def got_first(self):
        self.into(0, 1, 0)
        self.into(1, 3, 0)

    def first_step(self, forward):
        if forward:
            self.out(2, 1, 0, 0, "f", True)
        else:
            self.out(2, 3, 0, 1, "f", False)

    def got_second(self, j, uneven=False):
        self.into(3 + 3 * j, FIRST[j], 1)
        self.into(4 + 3 * j, FIRST[j], 3)

        def pass_on(cut):
            for df, dg, start, stop in ((FIRST[j], 1, 0, cut), (FIRST[j], 3, cut, 2 * self.half)):
                ref = self.buf.at[self.slot(df, dg), pl.ds(start, stop - start)]
                to = self.at.step(self.axes["g"], dg == 1)
                remote(ref, ref, self.send, self.recv.at[5 + 3 * j], sp=to).start()

        if uneven:
            for zl, cut in ((0, self.half // 2), (1, 3 * self.half // 2)):
                pl.when(self.at.zl == zl)(functools.partial(pass_on, cut))
        else:
            pass_on(self.half)
        self.across(FIRST[j], 1)
        self.across(FIRST[j], 3)

    def got_opposite(self):
        self.into(2, 2, 0)
        self.along_second(3)

    def got_far(self, j):
        self.into(5 + 3 * j, FIRST[j], 2)
        self.across(FIRST[j], 2, 1)

    def from_other(self, far):
        ref = self.buf.at[pl.ds(0, 4 if far else 12)]
        remote(ref, ref, self.send, self.drecv.at[far], sp=self.at.other).wait_recv()

    def drain(self):
        ref = self.buf.at[pl.ds(0, 31)]
        remote(ref, ref, self.send, self.drecv.at[0], sp=self.at.other).wait_send()


class HalfGather:
    def __init__(self, at, buf, send, recv, drecv):
        self.at, self.buf, self.send, self.recv, self.drecv = at, buf, send, recv, drecv
        self.half = buf.shape[1] // 2

    def slot(self, dy, zo):
        return self.at.half_chip(dy, zo) * 2 + self.at.core

    def copy(self, ident, dy, zo, half, to):
        ref = self.buf.at[self.slot(dy, zo)]
        if half is not None:
            ref = self.buf.at[self.slot(dy, zo), pl.ds(half * self.half, self.half)]
        return remote(ref, ref, self.send, self.recv.at[ident], sp=to)

    def out(self, ident, dy, zo, half, to):
        self.copy(ident, dy, zo, half, to).start()

    def into(self, ident, dy, zo):
        self.copy(ident, dy, zo, None, self.at.other).wait_recv()

    def over(self, t, slot):
        ref = self.buf.at[slot]
        return remote(ref, ref, self.send, self.drecv.at[t], sp=self.at.other)

    def across(self, dy, zo):
        self.over(HALF_STEP_OF[dy, zo], self.slot(dy, zo)).start()

    def both_from_other(self, t):
        ref = self.buf.at[pl.ds(0, 2)]
        remote(ref, ref, self.send, self.drecv.at[t], sp=self.at.other).wait_recv()

    def ring_start(self, ident, zo):
        self.out(ident, 0, zo, None, self.at.step("y", True))
        self.out(ident + 1, 0, zo, None, self.at.step("y", False))

    def ring_middle(self, ident, zo, after=lambda dy: None):
        self.into(ident, 1, zo)
        self.out(ident + 2, 1, zo, 0, self.at.step("y", True))
        after(1)
        self.across(1, zo)
        self.into(ident + 1, 3, zo)
        self.out(ident + 2, 3, zo, 1, self.at.step("y", False))
        after(3)
        self.across(3, zo)

    def ring_end(self, ident, zo, after=lambda dy: None):
        self.into(ident + 2, 2, zo)
        after(2)
        self.across(2, zo)

    def drain(self):
        ref = self.buf.at[pl.ds(0, 15)]
        remote(ref, ref, self.send, self.recv.at[0], sp=self.at.other).wait_send()


def kernel(
    lam_in, sub_in, norm_in, conv_g_in, conv_u_in,
    q_in, k_in, v_in, wg_in, wu_in, wo_in, wd_in, res_in,
    out,
    lam, sub_gain, norm_gain, conv_g, conv_u, q_raw, k_raw, v_raw, q, kbuf, vbuf, wg, wu, wo, wd, res,
    m_s, l_s, acc, a_far, stat, stat_far, n_all, mid, hn, pre, hid, part, relay, parts, ended,
    lsem, send, krecv, kdrecv, wrecv, drecv, orecv, nrecv, xrecv, precv,
):
    at = Where()
    x, sp, core, other = at.x, at.sp, at.core, at.other
    rows = q.shape[1]
    own = rows // 4
    late = at.late == 1
    early = at.late == 0
    mine = at.half_chip(0, 0)

    barrier = pltpu.get_barrier_semaphore()
    after, before = lax.rem(sp + 1, 32), lax.rem(sp + 31, 32)
    for to in (other, at.step("y", True), at.step("y", False), at.step("z", True), at.step("z", False)):
        pl.semaphore_signal(barrier, inc=1, device_id={"sp": to}, device_id_type=MESH)
    for to in (after, before):
        for x_to in range(4):
            pl.semaphore_signal(barrier, inc=1, device_id={"sp": to, "tp": x_to}, device_id_type=MESH)
    xs = [lax.rem(x + d, 4) for d in range(4)]
    for to in xs[1:]:
        pl.semaphore_signal(barrier, inc=1, device_id={"tp": to}, device_id_type=MESH)

    loads = [
        pltpu.make_async_copy(src, dst, lsem.at[i])
        for i, (src, dst) in enumerate(
            (
                (k_in, k_raw), (v_in, v_raw), (q_in, q_raw), (wo_in, wo.at[x]), (wg_in, wg.at[sp]), (wu_in, wu.at[sp]),
                (wd_in, wd), (res_in, res.at[pl.ds(16, rows)]), (lam_in, lam), (sub_in, sub_gain),
                (norm_in, norm_gain), (conv_g_in, conv_g), (conv_u_in, conv_u),
            )
        )
    ]
    for load in loads[:3]:
        load.start()
    loads[0].wait()
    kbuf[mine * 2 + core] = k_raw[...].reshape(kbuf.shape[1:])
    for load in loads[3:6] + loads[7:]:
        load.start()
    with jax.named_scope("barrier"):
        pl.semaphore_wait(barrier, 16)

    keys = HalfGather(at, kbuf, send.at[0], krecv.at[0], kdrecv)
    vals = HalfGather(at, vbuf, send.at[1], krecv.at[1], kdrecv)
    gate = Gather(at, wg, "y", send.at[2], wrecv.at[0], drecv.at[0])
    up = Gather(at, wu, "z", send.at[3], wrecv.at[1], drecv.at[1])

    def key_on(dy):
        keys.out(3 + FIRST.index(dy), dy, 0, None, at.pair())

    def q_copy():
        return remote(q.at[0], q.at[1], send.at[9], orecv.at[0], sp=at.opposite())

    keys.ring_start(0, 0)
    loads[1].wait()
    vbuf[mine * 2 + core] = v_raw[...].reshape(vbuf.shape[1:])
    vals.out(0, 0, 0, None, at.pair())
    key_on(0)
    vals.ring_start(1, 0)
    keys.across(0, 0)
    vals.across(0, 0)
    loads[2].wait()
    q[0] = q_raw[...].reshape(q.shape[1:])

    @pl.when(late)
    def _():
        q_copy().start()

    def weights_along_z(forward):
        up.start_along("f", forward)
        gate.start_along("g", forward)

    loads[4].wait()
    loads[5].wait()
    for forward in (True, False):
        pl.when(at.zl == int(forward))(functools.partial(weights_along_z, forward))

    def weights_start():
        for forward in (True, False):
            up.start_along("g", forward)
            pl.when(at.zl == int(not forward))(functools.partial(weights_along_z, forward))
        gate.across(0, 0)
        up.across(0, 0)

    wo_half = wo.shape[1] // 2
    wo_quarter = wo_half // 2

    def wo_copy(ident, slot, start, size, to):
        ref = wo.at[slot, pl.ds(core * wo_half + start, size)]
        return remote(ref, ref, send.at[4], xrecv.at[ident], tp=to)

    def wo_over(slot):
        ref = wo.at[slot, pl.ds(core * wo_half, wo_half)]
        return remote(ref, ref, send.at[4], xrecv.at[3], sp=other)

    def res_copy(to):
        return remote(res.at[pl.ds(rows, 16)], res.at[pl.ds(0, 16)], send.at[6], xrecv.at[8], sp=to)

    def n_halo_copy(slot, to, x_to):
        return remote(
            n_all.at[slot, pl.ds(rows, 16)], n_all.at[slot, pl.ds(0, 16)], send.at[7], xrecv.at[9], sp=to, tp=x_to
        )

    loads[7].wait()
    loads[6].start()

    @pl.when(sp < 31)
    def _():
        res_copy(after).start()

    @pl.when(sp == 0)
    def _():
        res[:16, :] = jnp.zeros((16, res.shape[1]), BF16)
        n_all[:, :16, :] = jnp.zeros((4, 16, n_all.shape[2]), BF16)

    loads[3].wait()
    wo_copy(0, x, 0, wo_half, xs[1]).start()
    wo_copy(1, x, 0, wo_half, xs[3]).start()

    def wo_middle():
        wo_copy(0, xs[3], 0, wo_half, xs[1]).wait_recv()
        wo_copy(2, xs[3], 0, wo_quarter, xs[1]).start()
        wo_over(xs[3]).start()
        wo_copy(1, xs[1], 0, wo_half, xs[3]).wait_recv()
        wo_copy(2, xs[1], wo_quarter, wo_quarter, xs[3]).start()
        wo_over(xs[1]).start()

    def wo_end():
        wo_copy(2, xs[2], 0, wo_half, xs[1]).wait_recv()
        wo_over(xs[2]).start()

    def wo_wait():
        ref = wo.at[pl.ds(0, 3), pl.ds(0, wo_half)]
        remote(ref, ref, send.at[4], xrecv.at[3], sp=other).wait_recv()

    scale = 1.0 / math.sqrt(128.0) / math.log(2.0)

    def block(who, chip, masked):
        for j in range(4):
            h = j // 2
            kj = kbuf[pl.ds(chip * 2, 2), :, 128 * j : 128 * j + 128].reshape(2 * rows, 128)
            vj = vbuf[pl.ds(chip * 2, 2), :, 256 * h : 256 * h + 256].reshape(2 * rows, 256)
            s = lax.dot_general(
                q[who, :, 128 * j : 128 * j + 128], kj, (((1,), (1,)), ((), ())), preferred_element_type=F32
            )
            s = s * scale
            if masked:
                q_pos = lax.broadcasted_iota(jnp.int32, s.shape, 0) + core * rows
                s = jnp.where(lax.broadcasted_iota(jnp.int32, s.shape, 1) <= q_pos, s, -1e30)
            top = jnp.max(s, axis=1, keepdims=True)
            if masked:
                m_new = top
            else:
                m_old = m_s[4 * who + j][:, :1]
                m_new = jnp.maximum(m_old, top)
                alpha = jnp.exp2(m_old - m_new)
            p = jnp.exp2(s - m_new)
            part_sum = p[:, :128]
            for i in range(1, 2 * rows // 128):
                part_sum = part_sum + p[:, 128 * i : 128 * i + 128]
            pv = jnp.dot(p.astype(BF16), vj, preferred_element_type=F32)
            m_s[4 * who + j] = jnp.broadcast_to(m_new, (rows, 128))
            if masked:
                l_s[4 * who + j] = part_sum
                acc[4 * who + j] = pv
            else:
                l_s[4 * who + j] = l_s[4 * who + j] * alpha + part_sum
                acc[4 * who + j] = acc[4 * who + j] * alpha + pv

    @pl.when(early)
    def _():
        m_s[4:] = jnp.full((4, rows, 128), -1e30, F32)
        l_s[4:] = jnp.zeros((4, rows, 128), F32)
        acc[4:] = jnp.zeros((4, *acc.shape[1:]), F32)

    with jax.named_scope("own_wait"):
        keys.both_from_other(0)
    with jax.named_scope("own_block"):
        block(0, mine, True)

    def handler_0():
        keys.ring_middle(0, 0, key_on)
        vals.into(0, 0, 1)
        vals.ring_start(4, 1)
        for forward in (True, False):
            gate.start_along("f", forward)
        vals.across(0, 1)
        vals.ring_middle(1, 0)
        keys.into(3, 0, 1)
        keys.across(0, 1)

        @pl.when(early)
        def _():
            q_copy().wait_recv()

    def handler_2():
        keys.ring_end(0, 0, key_on)

    def gate_along_z(forward):
        gate.second_step(1, forward)
        gate.second_step(2, forward)

    def handler_4():
        vals.ring_middle(4, 1)
        for ident, dy in ((4, 1), (5, 3)):
            keys.into(ident, dy, 1)
            keys.across(dy, 1)

    def up_on(forward):
        up.into(0 if forward else 1, 1 if forward else 3, 0)
        up.first_step(forward)
        up.along_second(1 if forward else 2)

    def handler_5():
        gate.got_first()
        for forward in (True, False):
            pl.when(at.zl == int(forward))(functools.partial(gate_along_z, forward))
        weights_start()
        vals.ring_end(1, 0)
        for forward in (True, False):
            gate.first_step(forward)
        for forward in (True, False):
            pl.when(at.zl == int(not forward))(functools.partial(up_on, forward))
            pl.when(at.zl == int(not forward))(functools.partial(gate_along_z, forward))
        gate.across(FIRST[1], 0)
        gate.across(FIRST[2], 0)
        wo_middle()

    def handler_6():
        vals.ring_end(4, 1)
        keys.into(6, 2, 1)
        keys.across(2, 1)

    def step(t, carry):
        for when, handler in (
            (0, handler_0), (2, handler_2), (4, handler_4), (5, handler_5), (6, handler_6)
        ):

            @pl.when(t == when)
            def _():
                with jax.named_scope(handler.__name__):
                    handler()

        dy, zo = (pick(t, [d[i] for d in HALF_ORDER]) for i in (0, 1))
        chip = at.half_chip(dy, zo)

        @pl.when(t > 0)
        def _():
            with jax.named_scope("d2d_wait"):
                keys.both_from_other(t)

        @pl.when(early)
        def _():
            with jax.named_scope("far_block"):
                block(1, chip, False)

        @pl.when((chip < mine) & (late | (t < 4)))
        def _():
            with jax.named_scope("block"):
                block(0, chip, False)

        return carry

    def own_step(t, carry):
        dy, zo = (pick(t, [d[i] for d in HALF_ORDER]) for i in (0, 1))
        chip = at.half_chip(dy, zo)

        @pl.when(chip < mine)
        def _():
            with jax.named_scope("block"):
                block(0, chip, False)

        return carry

    lax.fori_loop(0, 8, step, 0)

    def stat_copy():
        return remote(stat, stat_far, send.at[10], orecv.at[1], sp=at.opposite())

    def a_copy(h):
        return remote(a_far.at[h], a_far.at[h], send.at[11], orecv.at[2 + h], sp=at.opposite())

    loads[8].wait()
    loads[9].wait()
    lanes = lax.broadcasted_iota(jnp.int32, (rows, 128), 1)
    base = 4 - 4 * at.late
    stats = jnp.zeros((rows, 128), F32)
    for j in range(4):
        total = jnp.sum(l_s[base + j], axis=1, keepdims=True)
        stats = jnp.where(lanes == j, m_s[base + j], jnp.where(lanes == 4 + j, total, stats))
    stat[...] = stats.T[:8]
    stat_copy().start()

    with jax.named_scope("w_first"):
        for forward in (True, False):
            pl.when(at.zl == int(forward))(functools.partial(up_on, forward))

    with jax.named_scope("stat_wait"):
        stat_copy().wait_recv()

    with jax.named_scope("blend"):
        here = jnp.concatenate([stat[...], jnp.zeros((120, rows), F32)], axis=0).T
        there = jnp.concatenate([stat_far[...], jnp.zeros((120, rows), F32)], axis=0).T
        for h in range(2):
            shares = []
            for j in (2 * h, 2 * h + 1):
                m_here, m_there = here[:, j : j + 1], there[:, j : j + 1]
                top = jnp.maximum(m_here, m_there)
                e_here, e_there = jnp.exp2(m_here - top), jnp.exp2(m_there - top)
                total = here[:, 4 + j : 5 + j] * e_here + there[:, 4 + j : 5 + j] * e_there
                shares.append(acc[base + j] * (e_here / total))
            a = shares[0] - lam[h] * shares[1]

            @pl.when(early)
            def _():
                a_far[h] = a.astype(BF16)
                a_copy(h).start()

            @pl.when(late)
            def _():
                acc[2 * h] = a

    @pl.when(early)
    def _():
        lax.fori_loop(4, 8, own_step, 0)

    with jax.named_scope("w_second"):
        gate.got_second(0)
        up.got_second(0)
        gate.got_opposite()
        up.got_opposite()

    def n_copy(ident, h, slot, start, size, to):
        ref = n_all.at[slot, pl.ds(16 + start, size), pl.ds(256 * h, 256)]
        return remote(ref, ref, send.at[5], nrecv.at[h, ident], tp=to)

    for h in range(2):

        @pl.when(late)
        def _():
            with jax.named_scope("a_wait"):
                a_copy(h).wait_recv()
            acc[2 * h] = acc[2 * h] + a_far[h].astype(F32)

        @pl.when(early)
        def _():
            mixed = []
            for j in (2 * h, 2 * h + 1):
                mixed.append(acc[j] / jnp.sum(l_s[j], axis=1, keepdims=True))
            acc[2 * h] = mixed[0] - lam[h] * mixed[1]

        a = acc[2 * h]
        square = jnp.mean(a * a, axis=1, keepdims=True)
        n = a * lax.rsqrt(square + EPS) * sub_gain[...] * (1.0 - LAMBDA_INIT)
        n_all[x, 16:, 256 * h : 256 * h + 256] = n.astype(BF16)
        n_copy(0, h, x, 0, rows, xs[1]).start()
        n_copy(1, h, x, 0, rows, xs[3]).start()

    @pl.when(sp < 31)
    def _():
        for x_to in range(4):
            n_halo_copy(x, after, x_to).start()

    with jax.named_scope("wo_end"):
        wo_end()
    with jax.named_scope("w_third"):
        for j in (1, 2):
            gate.got_second(j, uneven=True)
            up.got_second(j)
    with jax.named_scope("n_middle"):
        for h in range(2):
            n_copy(0, h, xs[3], 0, rows, xs[1]).wait_recv()
            n_copy(2, h, xs[3], 0, rows // 2, xs[1]).start()
            n_copy(1, h, xs[1], 0, rows, xs[3]).wait_recv()
            n_copy(2, h, xs[1], rows // 2, rows // 2, xs[3]).start()

    with jax.named_scope("w_fourth"):
        up.got_second(3)
        gate.got_second(3)

    @pl.when(sp > 0)
    def _():
        with jax.named_scope("halo_wait"):
            res_copy(before).wait_recv()
            ref = n_all.at[pl.ds(0, 4), pl.ds(0, 16)]
            remote(ref, ref, send.at[7], xrecv.at[9], sp=before).wait_recv()

    def project(slots, first):
        def body(i, carry):
            cols = pl.ds(pl.multiple_of(i * 256, 256), 256)
            sums = res[:, cols].astype(F32) if first else mid[:, cols]
            for slot in slots:
                sums = sums + jnp.dot(n_all[slot], wo[slot, :, cols], preferred_element_type=F32)
            mid[:, cols] = sums
            return carry

        lax.fori_loop(0, mid.shape[1] // 256, body, 0, unroll=2)

    with jax.named_scope("wo_wait"):
        wo_wait()
    with jax.named_scope("project"):
        project((x, xs[1], xs[3]), True)
    with jax.named_scope("n_wait"):
        for h in range(2):
            n_copy(2, h, xs[2], 0, rows, xs[1]).wait_recv()
    with jax.named_scope("project_last"):
        project((xs[2],), False)
    for load in loads[10:]:
        load.wait()
    with jax.named_scope("norm"):
        middle = mid[...]
        square = jnp.mean(middle * middle, axis=1, keepdims=True)
        hn[...] = (middle * lax.rsqrt(square + EPS) * norm_gain[...]).astype(BF16)
    feats = hn.shape[1]
    units = wg.shape[2]
    row, place = feats // 4, feats // 16

    def gate_part(dz, cols):
        z = lax.rem(at.z + dz, 4)
        return jnp.dot(
            hn[:, pl.ds(pl.multiple_of(z * row, row), row)], wg[pl.ds(z * 8, 8), :, cols].reshape(row, -1),
            preferred_element_type=F32,
        )

    def up_part(dy, cols):
        y = lax.rem(at.y + dy, 4)
        left = [hn[:, pl.ds(pl.multiple_of(z * row + y * place, place), place)] for z in range(4)]
        right = [wu[pl.ds(z * 8 + y * 2, 2), :, cols].reshape(place, -1) for z in range(4)]
        return jnp.dot(
            jnp.concatenate(left, axis=1), jnp.concatenate(right, axis=0), preferred_element_type=F32
        )

    def mix(g, taps):
        return taps[0:1] * pltpu.roll(g, 2, 0) + taps[1:2] * pltpu.roll(g, 1, 0) + taps[2:3] * g

    def feed_most(at_col, width):
        cols = pl.ds(at_col, width)
        for i, part_of in enumerate((gate_part, up_part)):
            pre[i, :, cols] = part_of(0, cols) + part_of(1, cols) + part_of(3, cols)

    def feed_last(at_col, width):
        cols = pl.ds(at_col, width)
        mixed = []
        for i, (part_of, taps) in enumerate(((gate_part, conv_g), (up_part, conv_u))):
            g = (pre[i, :, cols] + part_of(2, cols)).astype(BF16).astype(F32)
            mixed.append(mix(g, taps[:, cols])[16:])
        gc, uc = mixed
        hid[:, cols] = (gc * (0.5 + 0.5 * jnp.tanh(0.5 * gc)) * uc).astype(BF16)

    def feed(body, first=0, last=units):
        for start in range(first, last, 256):
            body(start, min(256, units - start))

    def far(*places):
        for j in places:
            gate.got_far(j)
            up.got_far(j)

    with jax.named_scope("w_far"):
        far(0, 1)
    with jax.named_scope("w_rest"):
        gate.from_other(0)
        up.from_other(0)
    with jax.named_scope("feed_most"):
        feed(feed_most, last=768)
        far(2)
        feed(feed_most, first=768)
    with jax.named_scope("w_fifth"):
        far(3)
    with jax.named_scope("w_over"):
        gate.from_other(1)
        up.from_other(1)
        loads[6].wait()
    with jax.named_scope("feed"):
        feed(feed_last)

    chunks = part.shape[2] // 512
    side = own // 2

    def cols_of(i):
        return pl.ds(pl.multiple_of(i * 512, 512), 512)

    def relay_copy(s, i, to):
        return remote(
            part.at[xs[2], pl.ds(s * side, side), cols_of(i)], relay.at[s, :, cols_of(i)],
            send.at[8], precv.at[0, i], tp=to,
        )

    def part_copy(s, i, to):
        return remote(
            part.at[to, :, cols_of(i)], parts.at[s, :, cols_of(i)], send.at[8], precv.at[1, i], tp=to
        )

    def arrived(buf, which, i):
        ref = buf.at[:, :, cols_of(i)]
        remote(ref, ref, send.at[8], precv.at[which, i], tp=xs[1]).wait_recv()

    def lower(i, carry):
        cols = cols_of(i)
        full = jnp.dot(hid[...], wd[:, cols], preferred_element_type=F32).astype(BF16)
        part[:, :, cols] = full.reshape(4, own, 512)
        relay_copy(0, i, xs[1]).start()
        relay_copy(1, i, xs[3]).start()
        return carry

    with jax.named_scope("lower"):
        lax.fori_loop(0, chunks, lower, 0, unroll=True)

    def pass_on(i, carry):
        cols = cols_of(i)
        arrived(relay, 0, i)
        for s, to in ((0, xs[1]), (1, xs[3])):
            half = pl.ds(s * side, side)
            both = part[to, half, cols].astype(F32) + relay[s, :, cols].astype(F32)
            part[to, half, cols] = both.astype(BF16)
            part_copy(s, i, to).start()
        return carry

    def sent(ref, which):
        remote(ref, ref, send.at[which], xrecv.at[0], sp=other).wait_send()

    with jax.named_scope("drain"):
        for gather in (keys, vals, gate, up):
            gather.drain()
        sent(wo.at[pl.ds(0, 3)], 4)
        sent(n_all.at[pl.ds(0, 3), pl.ds(0, rows)], 5)
        stat_copy().wait_send()

        @pl.when(sp < 31)
        def _():
            sent(hn.at[pl.ds(0, 16)], 6)
            sent(n_all.at[pl.ds(0, 4), pl.ds(0, 16)], 7)

        @pl.when(late)
        def _():
            q_copy().wait_send()

        @pl.when(early)
        def _():
            sent(a_far, 11)

    with jax.named_scope("pass_on"):
        lax.fori_loop(0, chunks, pass_on, 0)

    def finish(i, carry):
        cols = cols_of(i)
        arrived(parts, 1, i)
        sums = parts[0, :, cols].astype(F32) + parts[1, :, cols].astype(F32) + part[x, :, cols].astype(F32)
        middle = mid[pl.ds(pl.multiple_of(16 + x * own, 16), own), cols]
        ended[:, cols] = (middle + sums).astype(BF16)
        pltpu.make_async_copy(ended.at[:, cols], out.at[:, cols], lsem.at[i]).start()
        return carry

    with jax.named_scope("finish"):
        lax.fori_loop(0, chunks, finish, 0)

    sent(hn.at[pl.ds(0, 3 * own)], 8)
    for i in range(chunks):
        pltpu.make_async_copy(ended.at[:, cols_of(i)], out.at[:, cols_of(i)], lsem.at[i]).wait()


def local(
    residual, queries, key_rows, values, lambda_head, sub_gain, w_out, norm_gain, w_gate, w_up, conv_gate, conv_up,
    w_down,
):
    rows = queries.shape[0]
    d = residual.shape[1]
    own = rows // 4
    heads_wide = queries.shape[1] * values.shape[2]
    units = w_gate.shape[1]
    maps = queries.shape[1] * 2
    places = 32
    hbm = pl.BlockSpec(memory_space=pl.ANY)
    dma = pltpu.SemaphoreType.DMA
    call = pl.pallas_call(
        kernel,
        out_shape=jax.ShapeDtypeStruct((own, d), BF16),
        in_specs=[hbm] * 13,
        out_specs=hbm,
        scratch_shapes=[
            pltpu.SMEM(lambda_head.shape, F32),
            pltpu.VMEM((1, *sub_gain.shape), F32),
            pltpu.VMEM((1, d), F32),
            pltpu.VMEM(conv_gate.shape, F32),
            pltpu.VMEM(conv_up.shape, F32),
            pltpu.VMEM(queries.shape, BF16),
            pltpu.VMEM(key_rows.shape, BF16),
            pltpu.VMEM(values.shape, BF16),
            pltpu.VMEM((2, rows, 512), BF16),
            pltpu.VMEM((places // 2, rows, 512), BF16),
            pltpu.VMEM((places // 2, rows, 512), BF16),
            pltpu.VMEM((places, w_gate.shape[0], units), BF16),
            pltpu.VMEM((places, w_gate.shape[0], units), BF16),
            pltpu.VMEM((4, *w_out.shape), BF16),
            pltpu.VMEM(w_down.shape, BF16),
            pltpu.VMEM((rows + 16, d), BF16),
            pltpu.VMEM((2 * maps, rows, 128), F32),
            pltpu.VMEM((2 * maps, rows, 128), F32),
            pltpu.VMEM((2 * maps, rows, values.shape[2]), F32),
            pltpu.VMEM((2, rows, values.shape[2]), BF16),
            pltpu.VMEM((8, rows), F32),
            pltpu.VMEM((8, rows), F32),
            pltpu.VMEM((4, rows + 16, heads_wide), BF16),
            pltpu.VMEM((rows + 16, d), F32),
            pltpu.VMEM((rows + 16, d), BF16),
            pltpu.VMEM((2, rows + 16, units), F32),
            pltpu.VMEM((rows, units), BF16),
            pltpu.VMEM((4, own, d), BF16),
            pltpu.VMEM((2, own // 2, d), BF16),
            pltpu.VMEM((2, own, d), BF16),
            pltpu.VMEM((own, d), BF16),
            dma((13,)), dma((12,)), dma((2, 7)), dma((8,)), dma((2, 15)), dma((2, 2)), dma((4,)), dma((2, 3)), dma((10,)),
            dma((2, d // 512)),
        ],
        compiler_params=pltpu.CompilerParams(
            collective_id=0, has_side_effects=True, vmem_limit_bytes=67043328
        ),
    )
    return call(
        lambda_head, sub_gain[None], norm_gain[None], conv_gate, conv_up,
        queries, key_rows, values,
        w_gate, w_up, w_out, w_down, residual,
    )


def solution(mesh):
    placed = (
        P("sp", None),
        P("sp", "tp", None, None),
        P("sp", "tp", None, None),
        P("sp", "tp", None),
        P("tp"),
        P(),
        P("tp", None),
        P(),
        P("sp", "tp"),
        P("sp", "tp"),
        P(None, "tp"),
        P(None, "tp"),
        P("tp", None),
    )
    return jax.shard_map(
        local, mesh=mesh, in_specs=placed, out_specs=P(("sp", "tp"), None), check_vma=False
    )
```
